32 devices in a mesh: rep: 2 (over y), fs: 4 (over z), tp: 4 (over x, core).
Axes of the slice: x: 2, y: 2, z: 4, core: 2. Of those that a mesh axis runs over, the one named last changes fastest.
Arguments:
- activations: bfloat16 [3072, 2048], P(('rep', 'fs'), 'tp'), may hold values from -16 to 16
- norm_gain: float32 [2048], replicated, may hold values from 0.1 to 1.9
- query_weight: bfloat16 [2048, 512], P('fs', 'tp'), may hold values from -0.125 to 0.125
- key_weight: bfloat16 [2048, 512], P('fs', 'tp'), may hold values from -0.125 to 0.125
- value_weight: bfloat16 [2048, 512], P('fs', 'tp'), may hold values from -0.125 to 0.125
- gate_weight: bfloat16 [2048, 512], P('fs', 'tp'), may hold values from -0.125 to 0.125
- out_weight: bfloat16 [512, 2048], P('tp', 'fs'), may hold values from -0.25 to 0.25
- mlp_gain: float32 [2048], replicated, may hold values from 0.1 to 1.9
- up_weight: bfloat16 [2048, 8192], P('fs', 'tp'), may hold values from -0.125 to 0.125
- down_weight: bfloat16 [8192, 2048], P('tp', 'fs'), may hold values from -0.0625 to 0.0625
Outputs:
- layer_out: bfloat16 [3072, 2048], P(('rep', 'fs'), 'tp')
The draws below stay inside these ranges and needn't reach their ends.
All inputs are finite; a program needn't handle non-finite values.
Results may differ from the reference program's by a relative error of at most 0.012.
Values may be sent and summed in bfloat16 or wider, within the bound.
A program may use at most 64 MiB of HBM per device.

```python
import math
import jax
import jax.numpy as jnp
from jax import lax

D = 2048
FF = 8192
HEADS = 8
HEAD_DIM = 64
BLOCK = 64
SEQ_LEN = 128
TOKENS = 3072
N_TP = 4


def draw_activations(key, part):
    key_base, key_column, key_row = jax.random.split(jax.random.fold_in(key, 11), 3)
    column_index = jnp.arange(D, dtype=jnp.float32)
    column_scale = jnp.power(3.0, column_index / (D - 1)) * jnp.exp(jax.random.uniform(key_column, (D,), jnp.float32, -0.35, 0.35))
    base_draw = jax.random.normal(key_base, (TOKENS, D), jnp.float32)
    row_scale = jnp.exp(jax.random.uniform(key_row, (TOKENS, 1), jnp.float32, 0.0, math.log(4.0)))
    return jnp.clip(0.5 * base_draw * row_scale * column_scale[None, :], -16.0, 16.0).astype(jnp.bfloat16)


def level_of(key, shape, cuts, least, largest):
    loudness = 1.0
    for dim, shards_of in cuts:
        steps = jax.random.uniform(jax.random.fold_in(jax.random.fold_in(key, 6), dim), (shards_of,), jnp.float32, least / len(cuts), largest / len(cuts))
        loudness = loudness * jnp.repeat(jnp.exp(steps), shape[dim] // shards_of).reshape((-1,) + (1,) * (len(shape) - 1 - dim))
    return loudness


def noise(key, extent, scale, bound, cuts=(), kind=jnp.bfloat16):
    factor_of = level_of(key, extent, cuts, -0.22, 0.18) if cuts else 1.0
    values = jax.random.normal(key, extent, jnp.float32) * scale * factor_of
    return jnp.minimum(jnp.maximum(values, -bound), bound).astype(kind)


def setup_inputs(seed: int = 0) -> dict:
    streams_of = jax.random.split(jax.random.key(seed), 11)
    return {
        "activations": draw_activations(jax.random.fold_in(streams_of[10], 71), 0),
        "norm_gain": jnp.clip(1.0 + 0.18 * jax.random.normal(streams_of[1], (D,), jnp.float32), 0.1, 1.9),
        "query_weight": noise(streams_of[2], (D, HEADS * HEAD_DIM), D ** -0.5, 0.125, ((0, 4), (1, 4))),
        "key_weight": noise(streams_of[3], (D, HEADS * HEAD_DIM), D ** -0.5, 0.125, ((0, 4), (1, 4))),
        "value_weight": noise(streams_of[4], (D, HEADS * HEAD_DIM), D ** -0.5, 0.125, ((0, 4), (1, 4))),
        "gate_weight": noise(streams_of[5], (D, HEADS * HEAD_DIM), D ** -0.5, 0.125, ((0, 4), (1, 4))),
        "out_weight": noise(streams_of[6], (HEADS * HEAD_DIM, D), (HEADS * HEAD_DIM) ** -0.5, 0.25, ((0, 4), (1, 4))),
        "mlp_gain": jnp.clip(1.0 + 0.18 * jax.random.normal(streams_of[7], (D,), jnp.float32), 0.1, 1.9),
        "up_weight": noise(streams_of[8], (D, FF), D ** -0.5, 0.125, ((0, 4), (1, 4))),
        "down_weight": noise(streams_of[9], (FF, D), FF ** -0.5, 0.0625, ((0, 4), (1, 4))),
    }


EPSILON = 1e-06

def rms_norm(rows, gain):
    floats = rows.astype(jnp.float32)
    scaled = floats * lax.rsqrt(lax.optimization_barrier(jnp.mean(floats * floats, axis=-1, keepdims=True)) + EPSILON)
    return (scaled * gain.astype(jnp.float32)).astype(jnp.bfloat16)

def rotate(raw, cosine, sine, seqs, heads):
    half = HEAD_DIM // 2
    shaped = raw.reshape(seqs, SEQ_LEN, heads, HEAD_DIM)
    first, second = (shaped[..., :half], shaped[..., half:])
    return jnp.concatenate([first * cosine - second * sine, second * cosine + first * sine], axis=-1)

def retain(query_raw, key_raw, value_rows, gate_rows, first_head):
    tokens = query_raw.shape[0]
    heads = query_raw.shape[1] // HEAD_DIM
    seqs = tokens // SEQ_LEN
    blocks = SEQ_LEN // BLOCK
    half = HEAD_DIM // 2
    position = jnp.arange(SEQ_LEN, dtype=jnp.float32)
    freqs = 10000.0 ** (-jnp.arange(half, dtype=jnp.float32) / half)
    angle = position[:, None] * freqs[None, :]
    cosine = jnp.cos(angle)[:, None, :]
    sine = jnp.sin(angle)[:, None, :]
    shape_five = (seqs, blocks, BLOCK, heads, HEAD_DIM)
    queries = rotate(query_raw, cosine, sine, seqs, heads).astype(jnp.bfloat16).reshape(shape_five)
    key_block = (rotate(key_raw, cosine, sine, seqs, heads) * HEAD_DIM ** (-0.5)).astype(jnp.bfloat16).reshape(shape_five)
    value_block = value_rows.reshape(shape_five)
    head_index = first_head + jnp.arange(heads, dtype=jnp.float32)
    exponent = 5.0 + 4.0 * head_index / (HEADS - 1)
    log_gamma = jnp.log(1.0 - jnp.power(2.0, -exponent))
    offsets = jnp.arange(BLOCK, dtype=jnp.float32)
    distance = offsets[:, None] - offsets[None, :]
    decay_mask = jnp.where(distance[None] >= 0, jnp.exp(jnp.maximum(distance, 0.0)[None] * log_gamma[:, None, None]), 0.0)
    scores = jnp.einsum('snbhd,snchd->snhbc', queries.astype(jnp.float32), key_block.astype(jnp.float32))
    weights = (scores * decay_mask[None, None]).astype(jnp.bfloat16)
    inner = jnp.einsum('snhbc,snchd->snbhd', weights.astype(jnp.float32), value_block.astype(jnp.float32))
    query_decay = queries.astype(jnp.float32) * jnp.exp((offsets + 1.0)[:, None] * log_gamma[None, :])[:, :, None]
    key_decay = key_block.astype(jnp.float32) * jnp.exp((BLOCK - 1.0 - offsets)[:, None] * log_gamma[None, :])[:, :, None]
    block_decay = jnp.exp(BLOCK * log_gamma)[None, :, None, None]

    def advance(state, inputs):
        query_now, key_now, value_now = inputs
        carried = jnp.einsum('sbhd,shde->sbhe', query_now, state, precision=lax.Precision.HIGHEST)
        state = state * block_decay + jnp.einsum('sbhd,sbhe->shde', key_now, value_now, precision=lax.Precision.HIGHEST)
        return (state, carried)
    initial = jnp.zeros((seqs, heads, HEAD_DIM, HEAD_DIM), jnp.float32)
    _, cross = lax.scan(advance, initial, (jnp.moveaxis(query_decay, 1, 0), jnp.moveaxis(key_decay, 1, 0), jnp.moveaxis(value_block.astype(jnp.float32), 1, 0)))
    mixed = (inner + jnp.moveaxis(cross, 0, 1)).reshape(tokens, heads, HEAD_DIM)
    centred = mixed - lax.optimization_barrier(jnp.mean(mixed, axis=-1, keepdims=True))
    normed = centred * lax.rsqrt(lax.optimization_barrier(jnp.mean(centred * centred, axis=-1, keepdims=True)) + EPSILON)
    gated = normed * jax.nn.silu(gate_rows.reshape(tokens, heads, HEAD_DIM))
    return gated.reshape(tokens, heads * HEAD_DIM).astype(jnp.bfloat16)

def reference(activations, norm_gain, query_weight, key_weight, value_weight, gate_weight, out_weight, mlp_gain, up_weight, down_weight):
    normed = rms_norm(activations, norm_gain)
    query_raw = jnp.dot(normed, query_weight, preferred_element_type=jnp.float32)
    key_raw = jnp.dot(normed, key_weight, preferred_element_type=jnp.float32)
    value_rows = jnp.dot(normed, value_weight, preferred_element_type=jnp.float32).astype(jnp.bfloat16)
    gate_rows = jnp.dot(normed, gate_weight, preferred_element_type=jnp.float32)
    retained = retain(query_raw, key_raw, value_rows, gate_rows, 0.0)
    branch = jnp.dot(retained, out_weight, preferred_element_type=jnp.float32)
    middle = (activations.astype(jnp.float32) + branch).astype(jnp.bfloat16)
    second = rms_norm(middle, mlp_gain)
    hidden = jnp.square(jax.nn.relu(jnp.dot(second, up_weight, preferred_element_type=jnp.float32))).astype(jnp.bfloat16)
    group_width = FF // N_TP
    hidden_parts = jnp.moveaxis(hidden.reshape(hidden.shape[0], N_TP, group_width), 1, 0)
    down_parts = down_weight.reshape(N_TP, group_width, D)

    def accumulate(running, inputs):
        part_rows, part_weight = inputs
        rounded = lax.optimization_barrier(jnp.dot(part_rows, part_weight, preferred_element_type=jnp.float32).astype(jnp.bfloat16))
        return (running + rounded.astype(jnp.float32), None)
    summed, _ = lax.scan(accumulate, jnp.zeros((hidden.shape[0], D), jnp.float32), (hidden_parts, down_parts))
    return (middle.astype(jnp.float32) + summed).astype(jnp.bfloat16)
```

```python
import functools

import jax
import jax.numpy as jnp
import numpy as np
from jax import lax
from jax.experimental import pallas as pl
from jax.experimental.pallas import tpu as pltpu
from jax.sharding import PartitionSpec as P

HEADS = 8
HEAD_DIM = 64
SEQ_LEN = 128
EPSILON = 1e-06
MESH = pl.DeviceIdType.MESH
BF16 = jnp.bfloat16
F32 = jnp.float32


def tables(head_width):
    half = HEAD_DIM // 2
    freqs = np.float32(10000.0) ** (-np.arange(half, dtype=np.float32) / np.float32(half))
    angle = np.arange(SEQ_LEN, dtype=np.float32)[:, None] * freqs[None, :]
    lane = np.arange(2 * head_width)
    scale = np.where(lane < head_width, 1.0, HEAD_DIM**-0.5).astype(np.float32)
    sign = np.where(lane % HEAD_DIM < half, -1.0, 1.0).astype(np.float32)
    cosine = np.cos(angle)[:, lane % half] * scale
    sine = np.sin(angle)[:, lane % half] * scale * sign
    exponent = np.float32(5.0) + np.float32(4.0) * np.arange(HEADS, dtype=np.float32) / np.float32(HEADS - 1)
    log_gamma = np.log(np.float32(1.0) - np.power(np.float32(2.0), -exponent))
    place = np.arange(SEQ_LEN, dtype=np.float32)
    distance = place[:, None] - place[None, :]
    decay = np.where(
        distance[None] >= 0,
        np.exp(np.maximum(distance, 0.0)[None] * log_gamma[:, None, None]),
        0.0,
    )
    return cosine.astype(np.float32), sine.astype(np.float32), decay.astype(np.float32)


class Plan:
    def __init__(self):
        self.size = 0

    def take(self, count):
        base = self.size
        self.size += count
        return base


def build(mesh_shape, shapes):
    R, F, T = mesh_shape["rep"], mesh_shape["fs"], mesh_shape["tp"]
    X, HF, Q = T // 2, F // 2, F // T
    n, dc = shapes["activations"]
    dep, hw = shapes["query_weight"]
    fw = shapes["up_weight"][1]
    D = dc * T
    hid = fw // 2
    seqs = n // SEQ_LEN
    local_heads = hw // HEAD_DIM
    n_small = 4 if hw % 128 == 0 else 1
    sw = 4 * hw // n_small

    plan = Plan()
    L_ACT, L_OUT, L_UP, L_DOWN, L_DECAY, L_SMALL = (
        plan.take(1),
        plan.take(1),
        plan.take(1),
        plan.take(1),
        plan.take(1),
        plan.take(n_small),
    )

    class Spread:
        def __init__(self):
            self.send, self.recv = plan.take(2 * X - 1), plan.take(T)

    act_spread = Spread()
    ret_spread = [Spread() for _ in range(seqs)]
    mid_spread = [Spread() for _ in range(2)]
    mid_z = (plan.take(1), plan.take(1))
    om_send, om_recv = plan.take((T - 1) * Q), plan.take(T * Q)

    class Stream:
        def __init__(self):
            self.zs, self.zf, self.zr = plan.take(max(F, 3)), plan.take(F), plan.take(F)
            self.ys, self.yr = plan.take(F * R), plan.take(F * R)

    qkv_stream, out_stream, up_stream, down_stream = Stream(), Stream(), Stream(), Stream()
    ps, pr = plan.take(2 * F), plan.take(2 * F)
    xs, xr = plan.take(2 * F), plan.take(2 * max(X - 1, 1) * Q)
    fz_s, fz_r = plan.take(Q), plan.take(Q)

    def kernel(*refs):
        act = refs[0]
        small = refs[1 : 1 + n_small]
        (out_w, up_w, down_w, gain1, gain2, cosine, sine, decay_all, result) = refs[1 + n_small : 10 + n_small]
        (
            act_full,
            normed,
            wbuf,
            proj,
            decay,
            og,
            om,
            ret,
            mid,
            second,
            upb,
            dnb,
            acc,
            hidden,
            pf,
            pbuf,
            srecv,
            tot,
            xrecv,
            zsnd,
            zrecv,
            sem,
        ) = refs[10 + n_small :]
        r, f, t = lax.axis_index("rep"), lax.axis_index("fs"), lax.axis_index("tp")
        x, c = t // 2, t % 2
        sib = 2 * x + 1 - c
        h = f // HF
        partner = (f + HF) % F

        def order(k):
            g = h * (F - 1 - f) + (1 - h) * f
            past = (k + 2 * F - 2 * g - 1) // (2 * F)
            odd = k % 2
            near = g + odd * ((k + 1) // 2) - (1 - odd) * (k // 2)
            s = past * k + (1 - past) * near
            return h * (F - 1 - s) + (1 - h) * s

        def at(i):
            return sem.at[i]

        def remote(src, dst, send, recv, **where):
            return pltpu.make_async_remote_copy(
                src_ref=src,
                dst_ref=dst,
                send_sem=at(send),
                recv_sem=at(recv),
                device_id=where,
                device_id_type=MESH,
            )

        def local(src, dst, i):
            return pltpu.make_async_copy(src, dst, at(i))

        def span(start, size, unit):
            return pl.ds(pl.multiple_of(start, unit), size)

        def act_block(s):
            return act_full.at[:, span(s * dc, dc, dc)]

        def mid_block(g, s):
            return mid.at[g, :, span(s * dc, dc, dc)]

        def ret_block(j, s):
            return ret.at[s, pl.ds(j * SEQ_LEN, SEQ_LEN), :]

        def qkv_part(s, part):
            rows = dep // R
            return wbuf.at[span(s * dep + part * rows, rows, rows), :]

        def out_part(s, part):
            rows = hw // R
            return og.at[s, span(part * rows, rows, rows), :]

        def up_part(s, part):
            rows = dep // R
            return upb.at[span(s * dep + part * rows, rows, rows), :]

        def down_part(s, part):
            rows = hid // R
            return dnb.at[s, span(part * rows, rows, rows), :]

        def up_own(half):
            rows = dep // R
            return up_w.at[span(r * rows, rows, rows), span(half * hid, hid, hid)]

        def down_own(half):
            rows = hid // R
            return down_w.at[span(half * hid + r * rows, rows, rows), :]

        def spread_copies(sp, block, source):
            first = [remote(source, block(t), sp.send, sp.recv + t, tp=sib)]
            for j in range(1, X):
                first.append(remote(source, block(t), sp.send + j, sp.recv + t, tp=((x + j) % X) * 2 + c))
            return first

        def spread_start(sp, block, source):
            for copy in reversed(spread_copies(sp, block, source)):
                copy.start()

        def relay_copy(sp, block, j):
            s = ((x + X - j) % X) * 2 + c
            return remote(block(s), block(s), sp.send + X - 1 + j, sp.recv + s, tp=sib)

        def spread_relay(sp, block):
            for j in range(1, X):
                s = ((x + X - j) % X) * 2 + c
                remote(block(s), block(s), sp.send, sp.recv + s, tp=sib).wait_recv()
                relay_copy(sp, block, j).start()

        def spread_finish(sp, block):
            for j in range(X):
                s = ((x + X - j) % X) * 2 + 1 - c
                remote(block(s), block(s), sp.send, sp.recv + s, tp=sib).wait_recv()

        def spread_drain(sp, block, source):
            for copy in spread_copies(sp, block, source):
                copy.wait_send()
            for j in range(1, X):
                relay_copy(sp, block, j).wait_send()

        def y_copy(st, part, s, q):
            return remote(
                part(s, r), part(s, r), st.ys + s * R + q, st.yr + s * R + r, rep=(r + q) % R
            )

        def y_start(st, part, s):
            for q in range(1, R):
                y_copy(st, part, s, q).start()

        def y_wait(st, part, s):
            for q in range(1, R):
                other = (r + R - q) % R
                remote(
                    part(s, other), part(s, other), st.ys, st.yr + s * R + other, rep=other
                ).wait_recv()

        def z_wait(st, part, s):
            remote(part(s, r), part(s, r), st.zs, st.zr + s, fs=s).wait_recv()

        def direct_copy(st, part, k):
            return remote(part(f, r), part(f, r), st.zs + k, st.zr + f, fs=order(k))

        def own_copies(st, part, own):
            return (
                remote(own(1 - h), part(f, r), st.zs, st.zr + f, fs=HF - h),
                remote(own(h), part(f, r), st.zs + 1, st.zr + f, fs=(f + 1) % F),
                remote(own(h), part(f, r), st.zs + 2, st.zr + f, fs=(f + F - 1) % F),
            )

        def own_do(st, part, own, what):
            across, onward, back = own_copies(st, part, own)
            what(across)

            @pl.when(f % HF != HF - 1)
            def _():
                what(onward)

            @pl.when(f % HF != 0)
            def _():
                what(back)

        def forward_do(st, part, s, what):
            after = f + 2 * ((f - s + F) // F) - 1

            @pl.when((after + HF) // HF - 1 == h)
            def _():
                what(remote(part(s, r), part(s, r), st.zf + s, st.zr + s, fs=(after + F) % F))

        def pass_on(st, part, k):
            s = order(k)
            z_wait(st, part, s)
            forward_do(st, part, s, lambda copy: copy.start())
            y_start(st, part, s)

        head0 = t * local_heads
        loads = [local(act, act_block(t), L_ACT)]
        for i in range(n_small):
            loads.append(local(small[i], wbuf.at[span(f * dep, dep, dep), pl.ds(i * sw, sw)], L_SMALL + i))
        loads.append(local(out_w, og.at[f], L_OUT))
        loads.append(local(decay_all.at[pl.ds(head0, local_heads)], decay, L_DECAY))
        loads.append(local(up_w.at[:, span(h * hid, hid, hid)], upb.at[span(f * dep, dep, dep), :], L_UP))
        loads.append(local(down_w.at[span(h * hid, hid, hid), :], dnb.at[f], L_DOWN))
        for copy in loads:
            copy.start()

        barrier = pltpu.get_barrier_semaphore()
        for j in range(1, T):
            pl.semaphore_signal(barrier, inc=1, device_id={"tp": (t + j) % T}, device_id_type=MESH)
        for j in range(1, F):
            pl.semaphore_signal(barrier, inc=1, device_id={"fs": (f + j) % F}, device_id_type=MESH)
        for j in range(1, R):
            pl.semaphore_signal(barrier, inc=1, device_id={"rep": (r + j) % R}, device_id_type=MESH)
        pl.semaphore_wait(barrier, T + F + R - 3)

        spread_start(act_spread, act_block, act)
        for i in range(n_small):
            loads[1 + i].wait()
        for k in range(1, F):
            direct_copy(qkv_stream, qkv_part, k).start()
        loads[1 + n_small].wait()
        for k in range(1, F):
            direct_copy(out_stream, out_part, k).start()
        own_do(up_stream, up_part, up_own, lambda copy: copy.start())
        loads[0].wait()
        for copy in loads[2 + n_small :]:
            copy.wait()

        spread_relay(act_spread, act_block)
        spread_finish(act_spread, act_block)
        step = 64

        def norm_rows(source, gain, target):
            rows = source.astype(F32)
            mean = jnp.mean(rows * rows, axis=-1, keepdims=True)
            target[...] = (rows * lax.rsqrt(mean + EPSILON) * gain[...]).astype(BF16)

        def norm_first(i, carry):
            rows = span(i * step, step, step)
            norm_rows(act_full[rows, :], gain1, normed.at[rows, :])
            return carry

        lax.fori_loop(0, n // step, norm_first, 0)

        def project(k):
            s = order(k)
            part = jnp.dot(
                normed[:, span(s * dep, dep, dep)],
                wbuf[span(s * dep, dep, dep), :],
                preferred_element_type=F32,
            )
            if isinstance(k, int):
                proj[...] = part
            else:
                proj[...] += part

        project(0)

        def small_on(k, carry):
            s = order(k)
            z_wait(qkv_stream, qkv_part, s)
            y_start(qkv_stream, qkv_part, s)
            return carry

        lax.fori_loop(1, F, small_on, 0)

        def out_on(k, carry):
            s = order(k)
            z_wait(out_stream, out_part, s)
            y_start(out_stream, out_part, s)
            return carry

        lax.fori_loop(1, F, out_on, 0)

        def small_use(k, carry):
            y_wait(qkv_stream, qkv_part, order(k))
            project(k)
            return carry

        lax.fori_loop(1, F, small_use, 0)

        def out_take(k, carry):
            y_wait(out_stream, out_part, order(k))
            return carry

        lax.fori_loop(1, F, out_take, 0)

        def om_copy(j, i):
            to = (t + j) % T
            return remote(
                og.at[to * Q + i],
                om.at[i, span(t * hw, hw, hw), :],
                om_send + (j - 1) * Q + i,
                om_recv + t * Q + i,
                tp=to,
            )

        for j in range(1, T):
            for i in range(Q):
                om_copy(j, i).start()
        for i in range(Q):
            om[i, span(t * hw, hw, hw), :] = og[t * Q + i]

        lane = lax.broadcasted_iota(jnp.int32, (SEQ_LEN, 2 * hw), 1)
        first_half = lane % HEAD_DIM < HEAD_DIM // 2
        head_of = lax.broadcasted_iota(jnp.int32, (SEQ_LEN, hw), 1) // HEAD_DIM

        def of_head(values, i):
            return values if local_heads == 1 else jnp.where(head_of == i, values, 0.0)

        def head_mean(values):
            total = jnp.zeros_like(values)
            for i in range(local_heads):
                mean = jnp.sum(of_head(values, i), axis=-1, keepdims=True) * (1.0 / HEAD_DIM)
                total += of_head(jnp.broadcast_to(mean, values.shape), i)
            return total

        for j in range(seqs):
            rows = pl.ds(j * SEQ_LEN, SEQ_LEN)
            raw = proj[rows, : 2 * hw]
            turned = jnp.where(
                first_half,
                pltpu.roll(raw, 2 * hw - HEAD_DIM // 2, 1),
                pltpu.roll(raw, HEAD_DIM // 2, 1),
            )
            both = raw * cosine[...] + turned * sine[...]
            query, key = both[:, :hw], both[:, hw:].astype(BF16)
            value = proj[rows, 2 * hw : 3 * hw]
            gate = proj[rows, 3 * hw :]
            mixed = jnp.zeros((SEQ_LEN, hw), F32)
            for i in range(local_heads):
                scores = lax.dot_general(
                    of_head(query, i).astype(BF16), key, (((1,), (1,)), ((), ())), preferred_element_type=F32
                )
                weights = (scores * decay[i]).astype(BF16)
                mixed += jnp.dot(weights, of_head(value, i).astype(BF16), preferred_element_type=F32)
            centred = mixed - head_mean(mixed)
            spread_of = lax.rsqrt(head_mean(centred * centred) + EPSILON)
            ret[t, rows, :] = (centred * spread_of * (gate * jax.nn.sigmoid(gate))).astype(BF16)
            block = functools.partial(ret_block, j)
            spread_start(ret_spread[j], block, block(t))

        pass_on(up_stream, up_part, 1)

        for j in range(1, T):
            s = (t + T - j) % T
            for i in range(Q):
                block = om.at[i, span(s * hw, hw, hw), :]
                remote(block, block, om_send, om_recv + s * Q + i, tp=s).wait_recv()
        for j in range(seqs):
            spread_relay(ret_spread[j], functools.partial(ret_block, j))
        for j in range(seqs):
            block = functools.partial(ret_block, j)
            spread_finish(ret_spread[j], block)
            rows = pl.ds(j * SEQ_LEN, SEQ_LEN)
            for i in range(Q):
                branch = jnp.zeros((SEQ_LEN, dep), F32)
                for s in range(T):
                    branch += jnp.dot(
                        ret[s, rows, :], om[i, pl.ds(s * hw, hw), :], preferred_element_type=F32
                    )
                columns = span(t * dc + i * dep, dep, dep)
                mid[0, rows, columns] = (act_full[rows, columns].astype(F32) + branch).astype(BF16)
        mid_own = functools.partial(mid_block, 0)
        mid_other = functools.partial(mid_block, 1)
        spread_start(mid_spread[0], mid_own, mid_own(t))
        to_partner = remote(mid_own(t), mid_other(t), mid_z[0], mid_z[1], fs=partner)
        to_partner.start()
        own_do(down_stream, down_part, down_own, lambda copy: copy.start())

        def up_on(k, carry):
            pass_on(up_stream, up_part, k)
            return carry

        lax.fori_loop(2, F, up_on, 0)

        spread_relay(mid_spread[0], mid_own)
        spread_finish(mid_spread[0], mid_own)

        def norm_second(g):
            def body(i, carry):
                rows = span(i * step, step, step)
                norm_rows(mid[g, rows, :], gain2, second.at[g, rows, :])
                return carry

            lax.fori_loop(0, n // step, body, 0)

        norm_second(0)
        to_partner.wait_recv()
        spread_start(mid_spread[1], mid_other, mid_other(t))
        spread_relay(mid_spread[1], mid_other)
        spread_finish(mid_spread[1], mid_other)
        norm_second(1)

        def raise_by(k):
            s = order(k)
            for g in range(2):
                part = jnp.dot(
                    second[g, :, span(s * dep, dep, dep)],
                    upb[span(s * dep, dep, dep), :],
                    preferred_element_type=F32,
                )
                if isinstance(k, int):
                    acc[g] = part
                else:
                    acc[g] += part

        raise_by(0)

        def up_use(k, carry):
            y_wait(up_stream, up_part, order(k))
            raise_by(k)
            return carry

        lax.fori_loop(1, F, up_use, 0)
        for g in range(2):
            kept = jnp.maximum(acc[g], 0.0)
            hidden[g] = (kept * kept).astype(BF16)

        def where_to(k):
            s = order(k)
            return s, s // Q, s % Q

        def lower(k):
            s, td, i = where_to(k)
            xd, cd = td // 2, td % 2
            for g in (1, 0):
                pf[g] = jnp.dot(hidden[g], dnb[s], preferred_element_type=F32)

                @pl.when(c != cd)
                def _():
                    pbuf[s, g] = pf[g].astype(BF16)
                    remote(
                        pbuf.at[s, g], srecv.at[s, g], ps + 2 * s + g, pr + 2 * s + g, tp=sib
                    ).start()

            @pl.when(c == cd)
            def _():
                for g in (1, 0):
                    remote(
                        pbuf.at[s, g], srecv.at[s, g], ps + 2 * s + g, pr + 2 * s + g, tp=sib
                    ).wait_recv()
                    total = pf[g] + srecv[s, g].astype(F32)

                    @pl.when(x == xd)
                    def _():
                        tot[g, i] = total

                    @pl.when(x != xd)
                    def _():
                        pbuf[s, g] = total.astype(BF16)
                        x_copy(s, g).start()

        def x_copy(s, g):
            td, i = s // Q, s % Q
            away = (x + X - td // 2) % X
            slot = (away + X - 1) % X % max(X - 1, 1)
            return remote(
                pbuf.at[s, g],
                xrecv.at[slot, g, i],
                xs + 2 * s + g,
                xr + (slot * 2 + g) * Q + i,
                tp=(td // 2) * 2 + c,
            )

        def z_copy(i):
            return remote(zsnd.at[i], zrecv.at[i], fz_s + i, fz_r + i, fs=partner)

        def settle(k):
            s, td, i = where_to(k)

            @pl.when(td == t)
            def _():
                for g in (1, 0):
                    total = tot[g, i]
                    for slot in range(X - 1):
                        block = xrecv.at[slot, g, i]
                        remote(block, block, xs, xr + (slot * 2 + g) * Q + i, tp=sib).wait_recv()
                        total += xrecv[slot, g, i].astype(F32)
                    if g == 1:
                        zsnd[i] = total.astype(BF16)
                        z_copy(i).start()
                    else:
                        tot[0, i] = total

        lower(0)

        def down_use(k, carry):
            pass_on(down_stream, down_part, k)
            y_wait(down_stream, down_part, order(k))
            lower(k)
            settle(k - 1)
            return carry

        lax.fori_loop(1, F, down_use, 0)
        settle(F - 1)
        for i in range(Q):
            z_copy(i).wait_recv()
            columns = span(t * dc + i * dep, dep, dep)
            result[:, i * dep : (i + 1) * dep] = (
                mid[0, :, columns].astype(F32) + (tot[0, i] + zrecv[i].astype(F32))
            ).astype(BF16)

        spread_drain(act_spread, act_block, act)
        for j in range(seqs):
            block = functools.partial(ret_block, j)
            spread_drain(ret_spread[j], block, block(t))
        spread_drain(mid_spread[0], mid_own, mid_own(t))
        spread_drain(mid_spread[1], mid_other, mid_other(t))
        to_partner.wait_send()
        for j in range(1, T):
            for i in range(Q):
                om_copy(j, i).wait_send()
        for i in range(Q):
            z_copy(i).wait_send()
        own_do(up_stream, up_part, up_own, lambda copy: copy.wait_send())
        own_do(down_stream, down_part, down_own, lambda copy: copy.wait_send())

        def sent(k, carry):
            s = order(k)
            direct_copy(qkv_stream, qkv_part, k).wait_send()
            direct_copy(out_stream, out_part, k).wait_send()
            forward_do(up_stream, up_part, s, lambda copy: copy.wait_send())
            forward_do(down_stream, down_part, s, lambda copy: copy.wait_send())
            for st, part in (
                (qkv_stream, qkv_part),
                (out_stream, out_part),
                (up_stream, up_part),
                (down_stream, down_part),
            ):
                for q in range(1, R):
                    y_copy(st, part, s, q).wait_send()
            return carry

        lax.fori_loop(1, F, sent, 0)

        def summed(k, carry):
            s, td, i = where_to(k)
            for g in range(2):

                @pl.when(c != td % 2)
                def _():
                    remote(
                        pbuf.at[s, g], srecv.at[s, g], ps + 2 * s + g, pr + 2 * s + g, tp=sib
                    ).wait_send()

                @pl.when((c == td % 2) & (x != td // 2))
                def _():
                    x_copy(s, g).wait_send()

            return carry

        lax.fori_loop(0, F, summed, 0)

    vmem = pltpu.VMEM
    scratch = [
        vmem((n, D), BF16),
        vmem((n, D), BF16),
        vmem((D, 4 * hw), BF16),
        vmem((n, 4 * hw), F32),
        vmem((local_heads, SEQ_LEN, SEQ_LEN), F32),
        vmem((F, hw, dep), BF16),
        vmem((Q, T * hw, dep), BF16),
        vmem((T, n, hw), BF16),
        vmem((2, n, D), BF16),
        vmem((2, n, D), BF16),
        vmem((D, hid), BF16),
        vmem((F, hid, dep), BF16),
        vmem((2, n, hid), F32),
        vmem((2, n, hid), BF16),
        vmem((2, n, dep), F32),
        vmem((F, 2, n, dep), BF16),
        vmem((F, 2, n, dep), BF16),
        vmem((2, Q, n, dep), F32),
        vmem((max(X - 1, 1), 2, Q, n, dep), BF16),
        vmem((Q, n, dep), BF16),
        vmem((Q, n, dep), BF16),
        pltpu.SemaphoreType.DMA((plan.size,)),
    ]
    anywhere = pl.BlockSpec(memory_space=pl.ANY)
    in_vmem = pl.BlockSpec(memory_space=vmem)
    call = pl.pallas_call(
        kernel,
        name="layer",
        out_shape=jax.ShapeDtypeStruct((n, dc), BF16),
        in_specs=[anywhere] * (1 + n_small + 3) + [in_vmem] * 4 + [anywhere],
        out_specs=in_vmem,
        scratch_shapes=scratch,
        compiler_params=pltpu.CompilerParams(
            collective_id=0, has_side_effects=True, vmem_limit_bytes=62 * 1024 * 1024
        ),
    )
    return call, n_small


def solution(mesh):
    mesh_shape = dict(mesh.shape)

    def local(
        activations,
        norm_gain,
        query_weight,
        key_weight,
        value_weight,
        gate_weight,
        out_weight,
        mlp_gain,
        up_weight,
        down_weight,
    ):
        shapes = {
            "activations": activations.shape,
            "query_weight": query_weight.shape,
            "up_weight": up_weight.shape,
        }
        call, n_small = build(mesh_shape, shapes)
        small = (query_weight, key_weight, value_weight, gate_weight)
        if n_small == 1:
            small = (jnp.concatenate(small, axis=1),)
        cosine, sine, decay = tables(query_weight.shape[1])
        return call(
            activations,
            *small,
            out_weight,
            up_weight,
            down_weight,
            norm_gain.reshape(1, -1),
            mlp_gain.reshape(1, -1),
            jnp.asarray(cosine),
            jnp.asarray(sine),
            jnp.asarray(decay),
        )

    in_specs = (
        P(("rep", "fs"), "tp"),
        P(),
        P("fs", "tp"),
        P("fs", "tp"),
        P("fs", "tp"),
        P("fs", "tp"),
        P("tp", "fs"),
        P(),
        P("fs", "tp"),
        P("tp", "fs"),
    )
    return jax.shard_map(
        local, mesh=mesh, in_specs=in_specs, out_specs=P(("rep", "fs"), "tp"), check_vma=False
    )
```

```python
import functools

import jax
import jax.numpy as jnp
import numpy as np
from jax import lax
from jax.experimental import pallas as pl
from jax.experimental.pallas import tpu as pltpu
from jax.sharding import PartitionSpec as P

HEADS = 8
HEAD_DIM = 64
SEQ_LEN = 128
EPSILON = 1e-06
MESH = pl.DeviceIdType.MESH
BF16 = jnp.bfloat16
F32 = jnp.float32


def tables(head_width):
    half = HEAD_DIM // 2
    freqs = np.float32(10000.0) ** (-np.arange(half, dtype=np.float32) / np.float32(half))
    angle = np.arange(SEQ_LEN, dtype=np.float32)[:, None] * freqs[None, :]
    lane = np.arange(2 * head_width)
    scale = np.where(lane < head_width, 1.0, HEAD_DIM**-0.5).astype(np.float32)
    sign = np.where(lane % HEAD_DIM < half, -1.0, 1.0).astype(np.float32)
    cosine = np.cos(angle)[:, lane % half] * scale
    sine = np.sin(angle)[:, lane % half] * scale * sign
    exponent = np.float32(5.0) + np.float32(4.0) * np.arange(HEADS, dtype=np.float32) / np.float32(HEADS - 1)
    log_gamma = np.log(np.float32(1.0) - np.power(np.float32(2.0), -exponent))
    place = np.arange(SEQ_LEN, dtype=np.float32)
    distance = place[:, None] - place[None, :]
    decay = np.where(
        distance[None] >= 0,
        np.exp(np.maximum(distance, 0.0)[None] * log_gamma[:, None, None]),
        0.0,
    )
    return cosine.astype(np.float32), sine.astype(np.float32), decay.astype(np.float32)


class Plan:
    def __init__(self):
        self.size = 0

    def take(self, count):
        base = self.size
        self.size += count
        return base


def build(mesh_shape, shapes):
    R, F, T = mesh_shape["rep"], mesh_shape["fs"], mesh_shape["tp"]
    X, HF, Q = T // 2, F // 2, F // T
    n, dc = shapes["activations"]
    dep, hw = shapes["query_weight"]
    fw = shapes["up_weight"][1]
    D = dc * T
    hid = fw // 2
    seqs = n // SEQ_LEN
    local_heads = hw // HEAD_DIM
    n_small = 4 if hw % 128 == 0 else 1
    sw = 4 * hw // n_small

    plan = Plan()
    L_ACT, L_OUT, L_UP, L_DOWN, L_DECAY, L_SMALL = (
        plan.take(1),
        plan.take(1),
        plan.take(1),
        plan.take(R),
        plan.take(1),
        plan.take(n_small),
    )

    class Spread:
        def __init__(self):
            self.send, self.recv = plan.take(2 * X - 1), plan.take(T)

    act_spread = Spread()
    ret_spread = [Spread() for _ in range(seqs)]
    mid_spread = [Spread() for _ in range(2)]
    mid_z = (plan.take(1), plan.take(1))
    om_send, om_recv = plan.take((T - 1) * Q), plan.take(T * Q)

    class Stream:
        def __init__(self, chunks, line):
            self.chunks, self.line = chunks, line
            self.zs, self.zf, self.zr = (plan.take(3 * chunks), plan.take(F * chunks), plan.take(F * chunks))
            self.ys, self.yr = plan.take(F * R * chunks), plan.take(F * R * chunks)

    qkv_stream, out_stream = Stream(2, True), Stream(1, True)
    up_stream, down_stream = Stream(2, False), Stream(2, False)
    U = R if (dep // R) % 128 == 0 else 1
    uc = dep // U
    ps, pr = plan.take(2 * F * U), plan.take(2 * F * U)
    xs, xr = plan.take(2 * F * U), plan.take(2 * max(X - 1, 1) * Q * U)
    fz_s, fz_r = plan.take(Q * U), plan.take(Q * U)

    def kernel(*refs):
        act = refs[0]
        small = refs[1 : 1 + n_small]
        (out_w, up_w, down_w, gain1, gain2, cosine, sine, decay_all, result) = refs[1 + n_small : 10 + n_small]
        (
            act_full,
            normed,
            wbuf,
            proj,
            decay,
            og,
            om,
            ret,
            mid,
            second,
            upb,
            dnb,
            acc,
            hidden,
            pf,
            pbuf,
            srecv,
            tot,
            xrecv,
            zsnd,
            zrecv,
            sem,
        ) = refs[10 + n_small :]
        r, f, t = lax.axis_index("rep"), lax.axis_index("fs"), lax.axis_index("tp")
        x, c = t // 2, t % 2
        sib = 2 * x + 1 - c
        h = f // HF
        partner = (f + HF) % F

        def order(k):
            g = h * (F - 1 - f) + (1 - h) * f
            past = (k + 2 * F - 2 * g - 1) // (2 * F)
            odd = k % 2
            near = g + odd * ((k + 1) // 2) - (1 - odd) * (k // 2)
            s = past * k + (1 - past) * near
            return h * (F - 1 - s) + (1 - h) * s

        def at(i):
            return sem.at[i]

        def remote(src, dst, send, recv, **where):
            return pltpu.make_async_remote_copy(
                src_ref=src,
                dst_ref=dst,
                send_sem=at(send),
                recv_sem=at(recv),
                device_id=where,
                device_id_type=MESH,
            )

        def local(src, dst, i):
            return pltpu.make_async_copy(src, dst, at(i))

        def span(start, size, unit):
            return pl.ds(pl.multiple_of(start, unit), size)

        def act_block(s):
            return act_full.at[:, span(s * dc, dc, dc)]

        def mid_block(g, s):
            return mid.at[g, :, span(s * dc, dc, dc)]

        def ret_block(j, s):
            return ret.at[s, pl.ds(j * SEQ_LEN, SEQ_LEN), :]

        def rows_of(base, size, chunk, chunks):
            rows = size // chunks
            return span(base + chunk * rows, rows, rows)

        def qkv_part(s, part, ch):
            size = dep // R
            return wbuf.at[rows_of(s * dep + part * size, size, ch, qkv_stream.chunks), :]

        def out_part(s, part, ch):
            size = hw // R
            return og.at[s, rows_of(part * size, size, ch, out_stream.chunks), :]

        def up_part(s, part, ch):
            size = dep // R
            return upb.at[rows_of(s * dep + part * size, size, ch, up_stream.chunks), :]

        def down_part(s, part, ch):
            if U > 1:
                return dnb.at[s, part, rows_of(0, hid, ch, down_stream.chunks), :]
            size = hid // R
            return dnb.at[s, 0, rows_of(part * size, size, ch, down_stream.chunks), :]

        def qkv_own(half, ch):
            return qkv_part(f, r, ch)

        def out_own(half, ch):
            return out_part(f, r, ch)

        def up_own(half, ch):
            size = dep // R
            return up_w.at[rows_of(r * size, size, ch, up_stream.chunks), span(half * hid, hid, hid)]

        def down_own(half, ch):
            if U > 1:
                return down_w.at[rows_of(half * hid, hid, ch, down_stream.chunks), span(r * uc, uc, uc)]
            size = hid // R
            return down_w.at[rows_of(half * hid + r * size, size, ch, down_stream.chunks), :]

        def spread_copies(sp, block, source):
            first = [remote(source, block(t), sp.send, sp.recv + t, tp=sib)]
            for j in range(1, X):
                first.append(remote(source, block(t), sp.send + j, sp.recv + t, tp=((x + j) % X) * 2 + c))
            return first

        def spread_start(sp, block, source):
            for copy in reversed(spread_copies(sp, block, source)):
                copy.start()

        def relay_copy(sp, block, j):
            s = ((x + X - j) % X) * 2 + c
            return remote(block(s), block(s), sp.send + X - 1 + j, sp.recv + s, tp=sib)

        def spread_relay(sp, block):
            for j in range(1, X):
                s = ((x + X - j) % X) * 2 + c
                remote(block(s), block(s), sp.send, sp.recv + s, tp=sib).wait_recv()
                relay_copy(sp, block, j).start()

        def spread_finish(sp, block):
            for j in range(X):
                s = ((x + X - j) % X) * 2 + 1 - c
                remote(block(s), block(s), sp.send, sp.recv + s, tp=sib).wait_recv()

        def spread_drain(sp, block, source):
            for copy in spread_copies(sp, block, source):
                copy.wait_send()
            for j in range(1, X):
                relay_copy(sp, block, j).wait_send()

        deep = h * (f - HF) + (1 - h) * (HF - 1 - f)

        def y_copy(st, part, s, ch, q):
            block = part(s, r, ch)
            base = (s * R + q) * st.chunks + ch
            return remote(block, block, st.ys + base, st.yr + (s * R + r) * st.chunks + ch, rep=(r + q) % R)

        def y_wait(st, part, s):
            for q in range(1, R):
                other = (r + R - q) % R
                for ch in range(st.chunks):
                    block = part(s, other, ch)
                    remote(
                        block, block, st.ys, st.yr + (s * R + other) * st.chunks + ch, rep=other
                    ).wait_recv()

        def z_wait(st, part, s, ch):
            block = part(s, r, ch)
            remote(block, block, st.zs, st.zr + s * st.chunks + ch, fs=s).wait_recv()

        def along(st, part, own, what):
            size = F if st.line else HF
            for ch in range(st.chunks):
                source, target, arrived = own(h, ch), part(f, r, ch), st.zr + f * st.chunks + ch

                @pl.when(f % size != size - 1)
                def _():
                    what(remote(source, target, st.zs + ch, arrived, fs=(f + 1) % F))

                @pl.when(f % size != 0)
                def _():
                    what(remote(source, target, st.zs + st.chunks + ch, arrived, fs=(f + F - 1) % F))

        def across(st, part, own, what):
            for ch in range(st.chunks):
                what(
                    remote(
                        own(1 - h, ch),
                        part(f, r, ch),
                        st.zs + 2 * st.chunks + ch,
                        st.zr + f * st.chunks + ch,
                        fs=HF - h,
                    )
                )

        def forward(st, part, s, ch, what):
            after = f + 2 * ((f - s + F) // F) - 1
            size = F if st.line else HF

            @pl.when((after + size) // size - 1 == (0 if st.line else h))
            def _():
                block = part(s, r, ch)
                what(
                    remote(
                        block,
                        block,
                        st.zf + s * st.chunks + ch,
                        st.zr + s * st.chunks + ch,
                        fs=(after + F) % F,
                    )
                )

        def start(copy):
            copy.start()

        def leave(copy):
            copy.wait_send()

        def pass_on(st, part, k):
            s = order(k)
            for ch in range(st.chunks):
                z_wait(st, part, s, ch)
                forward(st, part, s, ch, start)
                for q in range(1, R):
                    y_copy(st, part, s, ch, q).start()

        def pass_range(st, part, first, last):
            def body(k, carry):
                pass_on(st, part, k)
                return carry

            if last > first:
                lax.fori_loop(first, last, body, 0)

        head0 = t * local_heads
        loads = [local(act, act_block(t), L_ACT)]
        for i in range(n_small):
            loads.append(local(small[i], wbuf.at[span(f * dep, dep, dep), pl.ds(i * sw, sw)], L_SMALL + i))
        loads.append(local(out_w, og.at[f], L_OUT))
        loads.append(local(decay_all.at[pl.ds(head0, local_heads)], decay, L_DECAY))
        loads.append(local(up_w.at[:, span(h * hid, hid, hid)], upb.at[span(f * dep, dep, dep), :], L_UP))
        for u in range(U):
            loads.append(
                local(down_w.at[span(h * hid, hid, hid), u * uc : (u + 1) * uc], dnb.at[f, u], L_DOWN + u)
            )
        for copy in loads:
            copy.start()

        barrier = pltpu.get_barrier_semaphore()
        for j in range(1, T):
            pl.semaphore_signal(barrier, inc=1, device_id={"tp": (t + j) % T}, device_id_type=MESH)
        for j in range(1, F):
            pl.semaphore_signal(barrier, inc=1, device_id={"fs": (f + j) % F}, device_id_type=MESH)
        for j in range(1, R):
            pl.semaphore_signal(barrier, inc=1, device_id={"rep": (r + j) % R}, device_id_type=MESH)
        pl.semaphore_wait(barrier, T + F + R - 3)

        spread_start(act_spread, act_block, act)
        for i in range(n_small):
            loads[1 + i].wait()
        along(qkv_stream, qkv_part, qkv_own, start)
        loads[1 + n_small].wait()
        along(out_stream, out_part, out_own, start)
        pass_on(qkv_stream, qkv_part, 1)
        pass_on(out_stream, out_part, 1)

        @pl.when(deep > 0)
        def _():
            along(up_stream, up_part, up_own, start)

        loads[0].wait()

        spread_relay(act_spread, act_block)
        spread_finish(act_spread, act_block)
        step = 64

        def norm_rows(source, gain, target):
            rows = source.astype(F32)
            mean = jnp.mean(rows * rows, axis=-1, keepdims=True)
            target[...] = (rows * lax.rsqrt(mean + EPSILON) * gain[...]).astype(BF16)

        def norm_first(i, carry):
            rows = span(i * step, step, step)
            norm_rows(act_full[rows, :], gain1, normed.at[rows, :])
            return carry

        lax.fori_loop(0, n // step, norm_first, 0)

        def project(k):
            s = order(k)
            part = jnp.dot(
                normed[:, span(s * dep, dep, dep)],
                wbuf[span(s * dep, dep, dep), :],
                preferred_element_type=F32,
            )
            if isinstance(k, int):
                proj[...] = part
            else:
                proj[...] += part

        project(0)

        def small_on(k, carry):
            pass_on(qkv_stream, qkv_part, k)
            pass_on(out_stream, out_part, k)
            return carry

        lax.fori_loop(2, F, small_on, 0)

        def own_weights(st, part, own):
            @pl.when(deep == 0)
            def _():
                along(st, part, own, start)

            @pl.when(deep > 0)
            def _():
                along(st, part, own, leave)

            across(st, part, own, start)

        own_weights(up_stream, up_part, up_own)

        def small_use(k, carry):
            y_wait(qkv_stream, qkv_part, order(k))
            project(k)
            y_wait(out_stream, out_part, order(k))
            return carry

        lax.fori_loop(1, F, small_use, 0)

        def om_copy(j, i):
            to = (t + j) % T
            return remote(
                og.at[to * Q + i],
                om.at[i, span(t * hw, hw, hw), :],
                om_send + (j - 1) * Q + i,
                om_recv + t * Q + i,
                tp=to,
            )

        for j in range(1, T):
            for i in range(Q):
                om_copy(j, i).start()
        for i in range(Q):
            om[i, span(t * hw, hw, hw), :] = og[t * Q + i]

        lane = lax.broadcasted_iota(jnp.int32, (SEQ_LEN, 2 * hw), 1)
        first_half = lane % HEAD_DIM < HEAD_DIM // 2
        head_of = lax.broadcasted_iota(jnp.int32, (SEQ_LEN, hw), 1) // HEAD_DIM

        def of_head(values, i):
            return values if local_heads == 1 else jnp.where(head_of == i, values, 0.0)

        def head_mean(values):
            total = jnp.zeros_like(values)
            for i in range(local_heads):
                mean = jnp.sum(of_head(values, i), axis=-1, keepdims=True) * (1.0 / HEAD_DIM)
                total += of_head(jnp.broadcast_to(mean, values.shape), i)
            return total

        loads[2 + n_small].wait()
        for j in range(seqs):
            rows = pl.ds(j * SEQ_LEN, SEQ_LEN)
            raw = proj[rows, : 2 * hw]
            turned = jnp.where(
                first_half,
                pltpu.roll(raw, 2 * hw - HEAD_DIM // 2, 1),
                pltpu.roll(raw, HEAD_DIM // 2, 1),
            )
            both = raw * cosine[...] + turned * sine[...]
            query, key = both[:, :hw], both[:, hw:].astype(BF16)
            value = proj[rows, 2 * hw : 3 * hw]
            gate = proj[rows, 3 * hw :]
            mixed = jnp.zeros((SEQ_LEN, hw), F32)
            for i in range(local_heads):
                scores = lax.dot_general(
                    of_head(query, i).astype(BF16), key, (((1,), (1,)), ((), ())), preferred_element_type=F32
                )
                weights = (scores * decay[i]).astype(BF16)
                mixed += jnp.dot(weights, of_head(value, i).astype(BF16), preferred_element_type=F32)
            centred = mixed - head_mean(mixed)
            spread_of = lax.rsqrt(head_mean(centred * centred) + EPSILON)
            ret[t, rows, :] = (centred * spread_of * (gate * jax.nn.sigmoid(gate))).astype(BF16)
            block = functools.partial(ret_block, j)
            spread_start(ret_spread[j], block, block(t))

        third = (F + 1) // 3
        pass_range(up_stream, up_part, 1, 1 + third)

        for j in range(1, T):
            s = (t + T - j) % T
            for i in range(Q):
                block = om.at[i, span(s * hw, hw, hw), :]
                remote(block, block, om_send, om_recv + s * Q + i, tp=s).wait_recv()
        for j in range(seqs):
            spread_relay(ret_spread[j], functools.partial(ret_block, j))
        for j in range(seqs):
            block = functools.partial(ret_block, j)
            spread_finish(ret_spread[j], block)
            rows = pl.ds(j * SEQ_LEN, SEQ_LEN)
            for i in range(Q):
                branch = jnp.zeros((SEQ_LEN, dep), F32)
                for s in range(T):
                    branch += jnp.dot(
                        ret[s, rows, :], om[i, pl.ds(s * hw, hw), :], preferred_element_type=F32
                    )
                columns = span(t * dc + i * dep, dep, dep)
                mid[0, rows, columns] = (act_full[rows, columns].astype(F32) + branch).astype(BF16)
        mid_own = functools.partial(mid_block, 0)
        mid_other = functools.partial(mid_block, 1)
        spread_start(mid_spread[0], mid_own, mid_own(t))
        to_partner = remote(mid_own(t), mid_other(t), mid_z[0], mid_z[1], fs=partner)
        to_partner.start()
        pass_range(up_stream, up_part, 1 + third, F - third)

        def norm_second(g):
            def body(i, carry):
                rows = span(i * step, step, step)
                norm_rows(mid[g, rows, :], gain2, second.at[g, rows, :])
                return carry

            lax.fori_loop(0, n // step, body, 0)

        to_partner.wait_recv()
        spread_start(mid_spread[1], mid_other, mid_other(t))
        spread_relay(mid_spread[0], mid_own)
        spread_finish(mid_spread[0], mid_own)
        norm_second(0)

        @pl.when(deep > 0)
        def _():
            along(down_stream, down_part, down_own, start)

        pass_range(up_stream, up_part, F - third, F)
        own_weights(down_stream, down_part, down_own)
        spread_relay(mid_spread[1], mid_other)
        spread_finish(mid_spread[1], mid_other)
        norm_second(1)

        def raise_by(k):
            s = order(k)
            for g in range(2):
                part = jnp.dot(
                    second[g, :, span(s * dep, dep, dep)],
                    upb[span(s * dep, dep, dep), :],
                    preferred_element_type=F32,
                )
                if isinstance(k, int):
                    acc[g] = part
                else:
                    acc[g] += part

        loads[3 + n_small].wait()
        raise_by(0)

        def up_use(k, carry):
            y_wait(up_stream, up_part, order(k))
            raise_by(k)
            return carry

        lax.fori_loop(1, F, up_use, 0)
        for g in range(2):
            kept = jnp.maximum(acc[g], 0.0)
            hidden[g] = (kept * kept).astype(BF16)

        def p_copy(s, u, g):
            i = (s * U + u) * 2 + g
            return remote(pbuf.at[s, u, g], srecv.at[s, u, g], ps + i, pr + i, tp=sib)

        def x_copy(s, u, g):
            td, i = s // Q, s % Q
            away = (x + X - td // 2) % X
            slot = (away + X - 1) % X % max(X - 1, 1)
            return remote(
                pbuf.at[s, u, g],
                xrecv.at[slot, g, i, u],
                xs + (s * U + u) * 2 + g,
                xr + ((slot * 2 + g) * Q + i) * U + u,
                tp=(td // 2) * 2 + c,
            )

        def z_copy(i, u):
            return remote(zsnd.at[i, u], zrecv.at[i, u], fz_s + i * U + u, fz_r + i * U + u, fs=partner)

        def unit(u):
            return (r + u) % U

        def lower(k, u):
            s = order(k)
            u = unit(u)
            td, i = s // Q, s % Q
            xd, cd = td // 2, td % 2
            for g in (1, 0):
                pf[g] = jnp.dot(hidden[g], dnb[s, u], preferred_element_type=F32)

                @pl.when(c != cd)
                def _():
                    pbuf[s, u, g] = pf[g].astype(BF16)
                    p_copy(s, u, g).start()

            @pl.when(c == cd)
            def _():
                for g in (1, 0):
                    p_copy(s, u, g).wait_recv()
                    total = pf[g] + srecv[s, u, g].astype(F32)

                    @pl.when(x == xd)
                    def _():
                        tot[g, i, u] = total

                    @pl.when(x != xd)
                    def _():
                        pbuf[s, u, g] = total.astype(BF16)
                        x_copy(s, u, g).start()

        def settle(k, u):
            s = order(k)
            u = unit(u)
            td, i = s // Q, s % Q

            @pl.when(td == t)
            def _():
                for g in (1, 0):
                    total = tot[g, i, u]
                    for slot in range(X - 1):
                        block = xrecv.at[slot, g, i, u]
                        remote(block, block, xs, xr + ((slot * 2 + g) * Q + i) * U + u, tp=sib).wait_recv()
                        total += xrecv[slot, g, i, u].astype(F32)
                    if g == 1:
                        zsnd[i, u] = total.astype(BF16)
                        z_copy(i, u).start()
                    else:
                        tot[0, i, u] = total

        pass_on(down_stream, down_part, 1)
        for copy in loads[4 + n_small :]:
            copy.wait()
        for u in range(U):
            lower(0, u)
        if U > 1:
            lower(1, 0)

        def down_use(k, carry):
            pass_on(down_stream, down_part, k)
            y_wait(down_stream, down_part, order(k - 1))
            if U > 1:
                settle(k - 2, 0)
                for u in range(1, U):
                    lower(k - 1, u)
                    settle(k - 2, u)
                lower(k, 0)
            else:
                lower(k - 1, 0)
                settle(k - 2, 0)
            return carry

        lax.fori_loop(2, F, down_use, 0)
        settle(F - 2, 0)
        y_wait(down_stream, down_part, order(F - 1))
        if U > 1:
            settle(F - 1, 0)
            for u in range(1, U):
                lower(F - 1, u)
                settle(F - 2, u)
                settle(F - 1, u)
        else:
            lower(F - 1, 0)
            settle(F - 1, 0)
        for i in range(Q):
            for u in range(U):
                z_copy(i, u).wait_recv()
                base = i * dep + u * uc
                columns = span(t * dc + base, uc, uc)
                result[:, base : base + uc] = (
                    mid[0, :, columns].astype(F32) + (tot[0, i, u] + zrecv[i, u].astype(F32))
                ).astype(BF16)

        spread_drain(act_spread, act_block, act)
        for j in range(seqs):
            block = functools.partial(ret_block, j)
            spread_drain(ret_spread[j], block, block(t))
        spread_drain(mid_spread[0], mid_own, mid_own(t))
        spread_drain(mid_spread[1], mid_other, mid_other(t))
        to_partner.wait_send()
        for j in range(1, T):
            for i in range(Q):
                om_copy(j, i).wait_send()
        for i in range(Q):
            for u in range(U):
                z_copy(i, u).wait_send()
        streams = (
            (qkv_stream, qkv_part, qkv_own),
            (out_stream, out_part, out_own),
            (up_stream, up_part, up_own),
            (down_stream, down_part, down_own),
        )
        for st, part, own in streams:
            if st.line:
                along(st, part, own, leave)
            else:

                @pl.when(deep == 0)
                def _():
                    along(st, part, own, leave)

                across(st, part, own, leave)

        def sent(k, carry):
            s = order(k)
            for st, part, own in streams:
                for ch in range(st.chunks):
                    forward(st, part, s, ch, leave)
                    for q in range(1, R):
                        y_copy(st, part, s, ch, q).wait_send()
            return carry

        lax.fori_loop(1, F, sent, 0)

        def summed(s, carry):
            td = s // Q
            for u in range(U):
                for g in range(2):

                    @pl.when(c != td % 2)
                    def _():
                        p_copy(s, u, g).wait_send()

                    @pl.when((c == td % 2) & (x != td // 2))
                    def _():
                        x_copy(s, u, g).wait_send()

            return carry

        lax.fori_loop(0, F, summed, 0)

    vmem = pltpu.VMEM
    scratch = [
        vmem((n, D), BF16),
        vmem((n, D), BF16),
        vmem((D, 4 * hw), BF16),
        vmem((n, 4 * hw), F32),
        vmem((local_heads, SEQ_LEN, SEQ_LEN), F32),
        vmem((F, hw, dep), BF16),
        vmem((Q, T * hw, dep), BF16),
        vmem((T, n, hw), BF16),
        vmem((2, n, D), BF16),
        vmem((2, n, D), BF16),
        vmem((D, hid), BF16),
        vmem((F, U, hid, uc), BF16),
        vmem((2, n, hid), F32),
        vmem((2, n, hid), BF16),
        vmem((2, n, uc), F32),
        vmem((F, U, 2, n, uc), BF16),
        vmem((F, U, 2, n, uc), BF16),
        vmem((2, Q, U, n, uc), F32),
        vmem((max(X - 1, 1), 2, Q, U, n, uc), BF16),
        vmem((Q, U, n, uc), BF16),
        vmem((Q, U, n, uc), BF16),
        pltpu.SemaphoreType.DMA((plan.size,)),
    ]
    anywhere = pl.BlockSpec(memory_space=pl.ANY)
    in_vmem = pl.BlockSpec(memory_space=vmem)
    call = pl.pallas_call(
        kernel,
        name="layer",
        out_shape=jax.ShapeDtypeStruct((n, dc), BF16),
        in_specs=[anywhere] * (1 + n_small + 3) + [in_vmem] * 4 + [anywhere],
        out_specs=in_vmem,
        scratch_shapes=scratch,
        compiler_params=pltpu.CompilerParams(
            collective_id=0, has_side_effects=True, vmem_limit_bytes=62 * 1024 * 1024
        ),
    )
    return call, n_small


def solution(mesh):
    mesh_shape = dict(mesh.shape)

    def local(
        activations,
        norm_gain,
        query_weight,
        key_weight,
        value_weight,
        gate_weight,
        out_weight,
        mlp_gain,
        up_weight,
        down_weight,
    ):
        shapes = {
            "activations": activations.shape,
            "query_weight": query_weight.shape,
            "up_weight": up_weight.shape,
        }
        call, n_small = build(mesh_shape, shapes)
        small = (query_weight, key_weight, value_weight, gate_weight)
        if n_small == 1:
            small = (jnp.concatenate(small, axis=1),)
        cosine, sine, decay = tables(query_weight.shape[1])
        return call(
            activations,
            *small,
            out_weight,
            up_weight,
            down_weight,
            norm_gain.reshape(1, -1),
            mlp_gain.reshape(1, -1),
            jnp.asarray(cosine),
            jnp.asarray(sine),
            jnp.asarray(decay),
        )

    in_specs = (
        P(("rep", "fs"), "tp"),
        P(),
        P("fs", "tp"),
        P("fs", "tp"),
        P("fs", "tp"),
        P("fs", "tp"),
        P("tp", "fs"),
        P(),
        P("fs", "tp"),
        P("tp", "fs"),
    )
    return jax.shard_map(
        local, mesh=mesh, in_specs=in_specs, out_specs=P(("rep", "fs"), "tp"), check_vma=False
    )
```

```python
import functools

import jax
import jax.numpy as jnp
import numpy as np
from jax import lax
from jax.experimental import pallas as pl
from jax.experimental.pallas import tpu as pltpu
from jax.sharding import PartitionSpec as P

HEADS = 8
HEAD_DIM = 64
SEQ_LEN = 128
EPSILON = 1e-06
MESH = pl.DeviceIdType.MESH
BF16 = jnp.bfloat16
F32 = jnp.float32


def tables(head_width):
    half = HEAD_DIM // 2
    freqs = np.float32(10000.0) ** (-np.arange(half, dtype=np.float32) / np.float32(half))
    angle = np.arange(SEQ_LEN, dtype=np.float32)[:, None] * freqs[None, :]
    lane = np.arange(2 * head_width)
    scale = np.where(lane < head_width, 1.0, HEAD_DIM**-0.5).astype(np.float32)
    sign = np.where(lane % HEAD_DIM < half, -1.0, 1.0).astype(np.float32)
    cosine = np.cos(angle)[:, lane % half] * scale
    sine = np.sin(angle)[:, lane % half] * scale * sign
    exponent = np.float32(5.0) + np.float32(4.0) * np.arange(HEADS, dtype=np.float32) / np.float32(HEADS - 1)
    log_gamma = np.log(np.float32(1.0) - np.power(np.float32(2.0), -exponent))
    place = np.arange(SEQ_LEN, dtype=np.float32)
    distance = place[:, None] - place[None, :]
    decay = np.where(
        distance[None] >= 0,
        np.exp(np.maximum(distance, 0.0)[None] * log_gamma[:, None, None]),
        0.0,
    )
    return cosine.astype(np.float32), sine.astype(np.float32), decay.astype(np.float32)


NEAR_FOUR = {
    ("begin",): (
        ("ps", 1),
        ("ps", 2),
    ),
    ("act",): (
        ("alu", 0),
    ),
    ("proj", 1): (
        ("acu", 0),
        ("ps", 3),
        ("alu", 1),
        ("pu", 2, 1),
        ("acu", 1),
        ("ald", 0),
        ("ald", 1),
    ),
    ("ret",): (
        ("pu", 3, 0),
        ("pu", 3, 1),
        ("pu", 2, 0),
    ),
    ("m0",): (
        ("pu", 1, 0),
        ("pu", 1, 1),
        ("acd", 0),
    ),
    ("tok",): (
        ("acd", 1),
    ),
    ("raise", 0): (
        ("pd", 2, 1),
    ),
    ("raise", 1): (
        ("pd", 3, 1),
    ),
    ("raise", 2): (
        ("pd", 1, 1),
    ),
    ("low", 0, 1): (
        ("pd", 1, 0),
        ("pd", 2, 0),
        ("pd", 3, 0),
    ),
}
DEEP_FOUR = {
    ("begin",): (
        ("ps", 1),
        ("alu", 0),
        ("alu", 1),
        ("acu", 0),
    ),
    ("act",): (
        ("acd", 1),
        ("acu", 1),
        ("ps", 2),
    ),
    ("proj", 2): (
        ("ps", 3),
        ("pu", 1, 0),
    ),
    ("ret",): (
        ("pu", 1, 1),
    ),
    ("mid",): (
        ("ald", 0),
        ("ald", 1),
        ("pd", 1, 0),
        ("pd", 1, 1),
        ("pu", 3, 0),
        ("pu", 3, 1),
    ),
    ("tok",): (
        ("pu", 2, 0),
        ("pu", 2, 1),
    ),
    ("m1",): (
        ("pd", 3, 1),
        ("acd", 0),
    ),
    ("raise", 2): (
        ("pd", 2, 1),
    ),
    ("low", 0, 1): (
        ("pd", 2, 0),
    ),
    ("low", 2, 0): (
        ("pd", 3, 0),
    ),
}


def spread_moves(planes, chunks):
    def every(name):
        return tuple((name, k, ch) for k in range(1, planes) for ch in range(chunks))

    def own(*names):
        return tuple((name, ch) for name in names for ch in range(chunks))

    return {
        ("begin",): tuple(("ps", k) for k in range(1, planes)) + own("alu", "acu"),
        ("mid",): every("pu") + own("ald", "acd"),
        ("tok",): every("pd"),
    }


def chain(planes, units):
    steps = [("begin",), ("act",)] + [("proj", k) for k in range(1, planes)]
    steps += [("ret",), ("mid",), ("m0",), ("tok",), ("m1",)] + [("raise", k) for k in range(planes)]
    pieces = [(k, u) for k in range(planes) for u in range(units)]
    behind = 2 if units > 1 else 1
    for i, piece in enumerate(pieces):
        steps.append(("low", *piece))
        if i >= behind:
            steps.append(("set", *pieces[i - behind]))
    steps += [("set", *piece) for piece in pieces[-behind:]]
    return steps + [("end",)]


class Plan:
    def __init__(self):
        self.size = 0

    def take(self, count):
        base = self.size
        self.size += count
        return base


def build(mesh_shape, shapes):
    R, F, T = mesh_shape["rep"], mesh_shape["fs"], mesh_shape["tp"]
    X, HF, Q = T // 2, F // 2, F // T
    n, dc = shapes["activations"]
    dep, hw = shapes["query_weight"]
    fw = shapes["up_weight"][1]
    D = dc * T
    hid = fw // 2
    seqs = n // SEQ_LEN
    local_heads = hw // HEAD_DIM
    n_small = 4 if hw % 128 == 0 else 1
    sw = 4 * hw // n_small

    plan = Plan()
    L_ACT, L_OUT, L_UP, L_DOWN, L_DECAY, L_SMALL = (
        plan.take(1),
        plan.take(1),
        plan.take(1),
        plan.take(R),
        plan.take(1),
        plan.take(n_small),
    )

    class Spread:
        def __init__(self):
            self.send, self.recv = plan.take(2 * X - 1), plan.take(T)

    act_spread = Spread()
    ret_spread = [Spread() for _ in range(seqs)]
    mid_spread = [Spread() for _ in range(2)]
    mid_z = (plan.take(1), plan.take(1))
    om_send, om_recv = plan.take((T - 1) * Q), plan.take(T * Q)

    class Stream:
        def __init__(self, chunks, line):
            self.chunks, self.line = chunks, line
            self.zs, self.zf, self.zr = (plan.take(3 * chunks), plan.take(F * chunks), plan.take(F * chunks))
            self.ys, self.yr = plan.take(F * R * chunks), plan.take(F * R * chunks)

    near_moves, deep_moves = (NEAR_FOUR, DEEP_FOUR) if F == 4 else (spread_moves(F, 2), spread_moves(F, 2))
    qkv_stream, out_stream = Stream(2, True), Stream(1, True)
    up_stream, down_stream = Stream(2, False), Stream(2, False)
    U = R if (dep // R) % 128 == 0 else 1
    uc = dep // U
    ps, pr = plan.take(2 * F * U), plan.take(2 * F * U)
    xs, xr = plan.take(2 * F * U), plan.take(2 * max(X - 1, 1) * Q * U)
    fz_s, fz_r = plan.take(Q * U), plan.take(Q * U)

    def kernel(*refs):
        act = refs[0]
        small = refs[1 : 1 + n_small]
        (out_w, up_w, down_w, gain1, gain2, cosine, sine, decay_all, result) = refs[1 + n_small : 10 + n_small]
        (
            act_full,
            normed,
            wbuf,
            proj,
            decay,
            og,
            om,
            ret,
            mid,
            second,
            upb,
            dnb,
            acc,
            hidden,
            pf,
            pbuf,
            srecv,
            tot,
            xrecv,
            zsnd,
            zrecv,
            sem,
        ) = refs[10 + n_small :]
        r, f, t = lax.axis_index("rep"), lax.axis_index("fs"), lax.axis_index("tp")
        x, c = t // 2, t % 2
        sib = 2 * x + 1 - c
        h = f // HF
        partner = (f + HF) % F

        def order(k):
            g = h * (F - 1 - f) + (1 - h) * f
            past = (k + 2 * F - 2 * g - 1) // (2 * F)
            odd = k % 2
            near = g + odd * ((k + 1) // 2) - (1 - odd) * (k // 2)
            s = past * k + (1 - past) * near
            return h * (F - 1 - s) + (1 - h) * s

        def at(i):
            return sem.at[i]

        def remote(src, dst, send, recv, **where):
            return pltpu.make_async_remote_copy(
                src_ref=src,
                dst_ref=dst,
                send_sem=at(send),
                recv_sem=at(recv),
                device_id=where,
                device_id_type=MESH,
            )

        def local(src, dst, i):
            return pltpu.make_async_copy(src, dst, at(i))

        def span(start, size, unit):
            return pl.ds(pl.multiple_of(start, unit), size)

        def act_block(s):
            return act_full.at[:, span(s * dc, dc, dc)]

        def mid_block(g, s):
            return mid.at[g, :, span(s * dc, dc, dc)]

        def ret_block(j, s):
            return ret.at[s, pl.ds(j * SEQ_LEN, SEQ_LEN), :]

        def rows_of(base, size, chunk, chunks):
            rows = size // chunks
            return span(base + chunk * rows, rows, rows)

        def qkv_part(s, part, ch):
            size = dep // R
            return wbuf.at[rows_of(s * dep + part * size, size, ch, qkv_stream.chunks), :]

        def out_part(s, part, ch):
            size = hw // R
            return og.at[s, rows_of(part * size, size, ch, out_stream.chunks), :]

        def up_part(s, part, ch):
            size = dep // R
            return upb.at[rows_of(s * dep + part * size, size, ch, up_stream.chunks), :]

        def down_part(s, part, ch):
            if U > 1:
                return dnb.at[s, part, rows_of(0, hid, ch, down_stream.chunks), :]
            size = hid // R
            return dnb.at[s, 0, rows_of(part * size, size, ch, down_stream.chunks), :]

        def qkv_own(half, ch):
            return qkv_part(f, r, ch)

        def out_own(half, ch):
            return out_part(f, r, ch)

        def up_own(half, ch):
            size = dep // R
            return up_w.at[rows_of(r * size, size, ch, up_stream.chunks), span(half * hid, hid, hid)]

        def down_own(half, ch):
            if U > 1:
                return down_w.at[rows_of(half * hid, hid, ch, down_stream.chunks), span(r * uc, uc, uc)]
            size = hid // R
            return down_w.at[rows_of(half * hid + r * size, size, ch, down_stream.chunks), :]

        def spread_copies(sp, block, source):
            first = [remote(source, block(t), sp.send, sp.recv + t, tp=sib)]
            for j in range(1, X):
                first.append(remote(source, block(t), sp.send + j, sp.recv + t, tp=((x + j) % X) * 2 + c))
            return first

        def spread_start(sp, block, source):
            for copy in reversed(spread_copies(sp, block, source)):
                copy.start()

        def relay_copy(sp, block, j):
            s = ((x + X - j) % X) * 2 + c
            return remote(block(s), block(s), sp.send + X - 1 + j, sp.recv + s, tp=sib)

        def spread_relay(sp, block):
            for j in range(1, X):
                s = ((x + X - j) % X) * 2 + c
                remote(block(s), block(s), sp.send, sp.recv + s, tp=sib).wait_recv()
                relay_copy(sp, block, j).start()

        def spread_finish(sp, block):
            for j in range(X):
                s = ((x + X - j) % X) * 2 + 1 - c
                remote(block(s), block(s), sp.send, sp.recv + s, tp=sib).wait_recv()

        def spread_drain(sp, block, source):
            for copy in spread_copies(sp, block, source):
                copy.wait_send()
            for j in range(1, X):
                relay_copy(sp, block, j).wait_send()

        deep = h * (f - HF) + (1 - h) * (HF - 1 - f)

        def y_copy(st, part, s, ch, q):
            block = part(s, r, ch)
            base = (s * R + q) * st.chunks + ch
            return remote(block, block, st.ys + base, st.yr + (s * R + r) * st.chunks + ch, rep=(r + q) % R)

        def y_wait(st, part, s):
            for q in range(1, R):
                other = (r + R - q) % R
                for ch in range(st.chunks):
                    block = part(s, other, ch)
                    remote(
                        block, block, st.ys, st.yr + (s * R + other) * st.chunks + ch, rep=other
                    ).wait_recv()

        def z_wait(st, part, s, ch):
            block = part(s, r, ch)
            remote(block, block, st.zs, st.zr + s * st.chunks + ch, fs=s).wait_recv()

        def along(st, part, own, what, chunks=None):
            size = F if st.line else HF
            for ch in range(st.chunks) if chunks is None else chunks:
                source, target, arrived = own(h, ch), part(f, r, ch), st.zr + f * st.chunks + ch

                @pl.when(f % size != size - 1)
                def _():
                    what(remote(source, target, st.zs + ch, arrived, fs=(f + 1) % F))

                @pl.when(f % size != 0)
                def _():
                    what(remote(source, target, st.zs + st.chunks + ch, arrived, fs=(f + F - 1) % F))

        def across(st, part, own, what, chunks=None):
            for ch in range(st.chunks) if chunks is None else chunks:
                what(
                    remote(
                        own(1 - h, ch),
                        part(f, r, ch),
                        st.zs + 2 * st.chunks + ch,
                        st.zr + f * st.chunks + ch,
                        fs=HF - h,
                    )
                )

        def forward(st, part, s, ch, what):
            after = f + 2 * ((f - s + F) // F) - 1
            size = F if st.line else HF

            @pl.when((after + size) // size - 1 == (0 if st.line else h))
            def _():
                block = part(s, r, ch)
                what(
                    remote(
                        block,
                        block,
                        st.zf + s * st.chunks + ch,
                        st.zr + s * st.chunks + ch,
                        fs=(after + F) % F,
                    )
                )

        def start(copy):
            copy.start()

        def leave(copy):
            copy.wait_send()

        def pass_on(st, part, k, chunks=None):
            s = order(k)
            for ch in range(st.chunks) if chunks is None else chunks:
                z_wait(st, part, s, ch)
                forward(st, part, s, ch, start)
                for q in range(1, R):
                    y_copy(st, part, s, ch, q).start()

        head0 = t * local_heads
        loads = [local(act, act_block(t), L_ACT)]
        for i in range(n_small):
            loads.append(local(small[i], wbuf.at[span(f * dep, dep, dep), pl.ds(i * sw, sw)], L_SMALL + i))
        loads.append(local(out_w, og.at[f], L_OUT))
        loads.append(local(decay_all.at[pl.ds(head0, local_heads)], decay, L_DECAY))
        loads.append(local(up_w.at[:, span(h * hid, hid, hid)], upb.at[span(f * dep, dep, dep), :], L_UP))
        for u in range(U):
            loads.append(
                local(down_w.at[span(h * hid, hid, hid), u * uc : (u + 1) * uc], dnb.at[f, u], L_DOWN + u)
            )
        for copy in loads:
            copy.start()

        barrier = pltpu.get_barrier_semaphore()
        for j in range(1, T):
            pl.semaphore_signal(barrier, inc=1, device_id={"tp": (t + j) % T}, device_id_type=MESH)
        for j in range(1, F):
            pl.semaphore_signal(barrier, inc=1, device_id={"fs": (f + j) % F}, device_id_type=MESH)
        for j in range(1, R):
            pl.semaphore_signal(barrier, inc=1, device_id={"rep": (r + j) % R}, device_id_type=MESH)
        pl.semaphore_wait(barrier, T + F + R - 3)

        def begin():
            spread_start(act_spread, act_block, act)
            for i in range(n_small):
                loads[1 + i].wait()
            along(qkv_stream, qkv_part, qkv_own, start)
            loads[1 + n_small].wait()
            along(out_stream, out_part, out_own, start)

        step = 64

        def norm_rows(source, gain, target):
            rows = source.astype(F32)
            mean = jnp.mean(rows * rows, axis=-1, keepdims=True)
            target[...] = (rows * lax.rsqrt(mean + EPSILON) * gain[...]).astype(BF16)

        def norm_first(i, carry):
            rows = span(i * step, step, step)
            norm_rows(act_full[rows, :], gain1, normed.at[rows, :])
            return carry

        def norm_act():
            loads[0].wait()
            spread_relay(act_spread, act_block)
            spread_finish(act_spread, act_block)
            lax.fori_loop(0, n // step, norm_first, 0)
            project(0)

        def project(k):
            s = order(k)
            part = jnp.dot(
                normed[:, span(s * dep, dep, dep)],
                wbuf[span(s * dep, dep, dep), :],
                preferred_element_type=F32,
            )
            if k == 0:
                proj[...] = part
            else:
                proj[...] += part

        def project_with(k):
            y_wait(qkv_stream, qkv_part, order(k))
            project(k)
            y_wait(out_stream, out_part, order(k))
            if k == F - 1:
                om_start()

        def om_copy(j, i):
            to = (t + j) % T
            return remote(
                og.at[to * Q + i],
                om.at[i, span(t * hw, hw, hw), :],
                om_send + (j - 1) * Q + i,
                om_recv + t * Q + i,
                tp=to,
            )

        def om_start():
            for j in range(1, T):
                for i in range(Q):
                    om_copy(j, i).start()
            for i in range(Q):
                om[i, span(t * hw, hw, hw), :] = og[t * Q + i]

        lane = lax.broadcasted_iota(jnp.int32, (SEQ_LEN, 2 * hw), 1)
        first_half = lane % HEAD_DIM < HEAD_DIM // 2
        head_of = lax.broadcasted_iota(jnp.int32, (SEQ_LEN, hw), 1) // HEAD_DIM

        def of_head(values, i):
            return values if local_heads == 1 else jnp.where(head_of == i, values, 0.0)

        def head_mean(values):
            total = jnp.zeros_like(values)
            for i in range(local_heads):
                mean = jnp.sum(of_head(values, i), axis=-1, keepdims=True) * (1.0 / HEAD_DIM)
                total += of_head(jnp.broadcast_to(mean, values.shape), i)
            return total

        def retain():
            loads[2 + n_small].wait()
            for j in range(seqs):
                rows = pl.ds(j * SEQ_LEN, SEQ_LEN)
                raw = proj[rows, : 2 * hw]
                turned = jnp.where(
                    first_half,
                    pltpu.roll(raw, 2 * hw - HEAD_DIM // 2, 1),
                    pltpu.roll(raw, HEAD_DIM // 2, 1),
                )
                both = raw * cosine[...] + turned * sine[...]
                query, key = both[:, :hw], both[:, hw:].astype(BF16)
                value = proj[rows, 2 * hw : 3 * hw]
                gate = proj[rows, 3 * hw :]
                mixed = jnp.zeros((SEQ_LEN, hw), F32)
                for i in range(local_heads):
                    scores = lax.dot_general(
                        of_head(query, i).astype(BF16), key, (((1,), (1,)), ((), ())), preferred_element_type=F32
                    )
                    weights = (scores * decay[i]).astype(BF16)
                    mixed += jnp.dot(weights, of_head(value, i).astype(BF16), preferred_element_type=F32)
                centred = mixed - head_mean(mixed)
                spread_of = lax.rsqrt(head_mean(centred * centred) + EPSILON)
                ret[t, rows, :] = (centred * spread_of * (gate * jax.nn.sigmoid(gate))).astype(BF16)
                block = functools.partial(ret_block, j)
                spread_start(ret_spread[j], block, block(t))

        mid_own = functools.partial(mid_block, 0)
        mid_other = functools.partial(mid_block, 1)
        to_partner = remote(mid_own(t), mid_other(t), mid_z[0], mid_z[1], fs=partner)

        def middle():
            for j in range(1, T):
                s = (t + T - j) % T
                for i in range(Q):
                    block = om.at[i, span(s * hw, hw, hw), :]
                    remote(block, block, om_send, om_recv + s * Q + i, tp=s).wait_recv()
            for j in range(seqs):
                spread_relay(ret_spread[j], functools.partial(ret_block, j))
            for j in range(seqs):
                block = functools.partial(ret_block, j)
                spread_finish(ret_spread[j], block)
                rows = pl.ds(j * SEQ_LEN, SEQ_LEN)
                for i in range(Q):
                    branch = jnp.zeros((SEQ_LEN, dep), F32)
                    for s in range(T):
                        branch += jnp.dot(
                            ret[s, rows, :], om[i, pl.ds(s * hw, hw), :], preferred_element_type=F32
                        )
                    columns = span(t * dc + i * dep, dep, dep)
                    mid[0, rows, columns] = (act_full[rows, columns].astype(F32) + branch).astype(BF16)
            spread_start(mid_spread[0], mid_own, mid_own(t))
            to_partner.start()

        def norm_second(g):
            def body(i, carry):
                rows = span(i * step, step, step)
                norm_rows(mid[g, rows, :], gain2, second.at[g, rows, :])
                return carry

            block = mid_other if g else mid_own
            spread_relay(mid_spread[g], block)
            spread_finish(mid_spread[g], block)
            lax.fori_loop(0, n // step, body, 0)

        def partner_rows():
            to_partner.wait_recv()
            spread_start(mid_spread[1], mid_other, mid_other(t))

        def raise_by(k):
            s = order(k)
            if k == 0:
                loads[3 + n_small].wait()
            else:
                y_wait(up_stream, up_part, s)
            for g in range(2):
                part = jnp.dot(
                    second[g, :, span(s * dep, dep, dep)],
                    upb[span(s * dep, dep, dep), :],
                    preferred_element_type=F32,
                )
                if k == 0:
                    acc[g] = part
                elif k < F - 1:
                    acc[g] += part
                else:
                    kept = jnp.maximum(acc[g] + part, 0.0)
                    hidden[g] = (kept * kept).astype(BF16)

        def p_copy(s, u, g):
            i = (s * U + u) * 2 + g
            return remote(pbuf.at[s, u, g], srecv.at[s, u, g], ps + i, pr + i, tp=sib)

        def x_copy(s, u, g):
            td, i = s // Q, s % Q
            away = (x + X - td // 2) % X
            slot = (away + X - 1) % X % max(X - 1, 1)
            return remote(
                pbuf.at[s, u, g],
                xrecv.at[slot, g, i, u],
                xs + (s * U + u) * 2 + g,
                xr + ((slot * 2 + g) * Q + i) * U + u,
                tp=(td // 2) * 2 + c,
            )

        def z_copy(i, u):
            return remote(zsnd.at[i, u], zrecv.at[i, u], fz_s + i * U + u, fz_r + i * U + u, fs=partner)

        def unit(u):
            return (r + u) % U

        def lower(k, u):
            s = order(k)
            if k == 0 and u == 0:
                for copy in loads[4 + n_small :]:
                    copy.wait()
            if k > 0 and u == U - 1:
                y_wait(down_stream, down_part, s)
            u = unit(u)
            td, i = s // Q, s % Q
            xd, cd = td // 2, td % 2
            for g in (1, 0):
                pf[g] = jnp.dot(hidden[g], dnb[s, u], preferred_element_type=F32)

                @pl.when(c != cd)
                def _():
                    pbuf[s, u, g] = pf[g].astype(BF16)
                    p_copy(s, u, g).start()

            @pl.when(c == cd)
            def _():
                for g in (1, 0):
                    p_copy(s, u, g).wait_recv()
                    total = pf[g] + srecv[s, u, g].astype(F32)

                    @pl.when(x == xd)
                    def _():
                        tot[g, i, u] = total

                    @pl.when(x != xd)
                    def _():
                        pbuf[s, u, g] = total.astype(BF16)
                        x_copy(s, u, g).start()

        def settle(k, u):
            s = order(k)
            u = unit(u)
            td, i = s // Q, s % Q

            @pl.when(td == t)
            def _():
                for g in (1, 0):
                    total = tot[g, i, u]
                    for slot in range(X - 1):
                        block = xrecv.at[slot, g, i, u]
                        remote(block, block, xs, xr + ((slot * 2 + g) * Q + i) * U + u, tp=sib).wait_recv()
                        total += xrecv[slot, g, i, u].astype(F32)
                    if g == 1:
                        zsnd[i, u] = total.astype(BF16)
                        z_copy(i, u).start()
                    else:
                        tot[0, i, u] = total

        def finish():
            for i in range(Q):
                for u in range(U):
                    z_copy(i, u).wait_recv()
                    base = i * dep + u * uc
                    columns = span(t * dc + base, uc, uc)
                    result[:, base : base + uc] = (
                        mid[0, :, columns].astype(F32) + (tot[0, i, u] + zrecv[i, u].astype(F32))
                    ).astype(BF16)

        near = deep == 0
        steps = {
            "begin": begin,
            "act": norm_act,
            "proj": project_with,
            "ret": retain,
            "mid": middle,
            "m0": lambda: norm_second(0),
            "tok": partner_rows,
            "m1": lambda: norm_second(1),
            "raise": raise_by,
            "low": lower,
            "set": settle,
            "end": finish,
        }

        def small_on(k):
            pass_on(qkv_stream, qkv_part, k)
            pass_on(out_stream, out_part, k)

        moves = {
            "ps": small_on,
            "alu": lambda ch: along(up_stream, up_part, up_own, start, (ch,)),
            "acu": lambda ch: across(up_stream, up_part, up_own, start, (ch,)),
            "ald": lambda ch: along(down_stream, down_part, down_own, start, (ch,)),
            "acd": lambda ch: across(down_stream, down_part, down_own, start, (ch,)),
            "pu": lambda k, ch: pass_on(up_stream, up_part, k, (ch,)),
            "pd": lambda k, ch: pass_on(down_stream, down_part, k, (ch,)),
        }
        for name, *place in chain(F, U):
            steps[name](*place)
            for here, table in ((near, near_moves), (deep > 0, deep_moves)):
                todo = table.get((name, *place), ())
                if todo:

                    @pl.when(here)
                    def _():
                        for move, *which in todo:
                            moves[move](*which)

        spread_drain(act_spread, act_block, act)
        for j in range(seqs):
            block = functools.partial(ret_block, j)
            spread_drain(ret_spread[j], block, block(t))
        spread_drain(mid_spread[0], mid_own, mid_own(t))
        spread_drain(mid_spread[1], mid_other, mid_other(t))
        to_partner.wait_send()
        for j in range(1, T):
            for i in range(Q):
                om_copy(j, i).wait_send()
        for i in range(Q):
            for u in range(U):
                z_copy(i, u).wait_send()
        streams = (
            (qkv_stream, qkv_part, qkv_own),
            (out_stream, out_part, out_own),
            (up_stream, up_part, up_own),
            (down_stream, down_part, down_own),
        )
        for st, part, own in streams:
            along(st, part, own, leave)
            if not st.line:
                across(st, part, own, leave)

        def sent(k, carry):
            s = order(k)
            for st, part, own in streams:
                for ch in range(st.chunks):
                    forward(st, part, s, ch, leave)
                    for q in range(1, R):
                        y_copy(st, part, s, ch, q).wait_send()
            return carry

        lax.fori_loop(1, F, sent, 0)

        def summed(s, carry):
            td = s // Q
            for u in range(U):
                for g in range(2):

                    @pl.when(c != td % 2)
                    def _():
                        p_copy(s, u, g).wait_send()

                    @pl.when((c == td % 2) & (x != td // 2))
                    def _():
                        x_copy(s, u, g).wait_send()

            return carry

        lax.fori_loop(0, F, summed, 0)

    vmem = pltpu.VMEM
    scratch = [
        vmem((n, D), BF16),
        vmem((n, D), BF16),
        vmem((D, 4 * hw), BF16),
        vmem((n, 4 * hw), F32),
        vmem((local_heads, SEQ_LEN, SEQ_LEN), F32),
        vmem((F, hw, dep), BF16),
        vmem((Q, T * hw, dep), BF16),
        vmem((T, n, hw), BF16),
        vmem((2, n, D), BF16),
        vmem((2, n, D), BF16),
        vmem((D, hid), BF16),
        vmem((F, U, hid, uc), BF16),
        vmem((2, n, hid), F32),
        vmem((2, n, hid), BF16),
        vmem((2, n, uc), F32),
        vmem((F, U, 2, n, uc), BF16),
        vmem((F, U, 2, n, uc), BF16),
        vmem((2, Q, U, n, uc), F32),
        vmem((max(X - 1, 1), 2, Q, U, n, uc), BF16),
        vmem((Q, U, n, uc), BF16),
        vmem((Q, U, n, uc), BF16),
        pltpu.SemaphoreType.DMA((plan.size,)),
    ]
    anywhere = pl.BlockSpec(memory_space=pl.ANY)
    in_vmem = pl.BlockSpec(memory_space=vmem)
    call = pl.pallas_call(
        kernel,
        name="layer",
        out_shape=jax.ShapeDtypeStruct((n, dc), BF16),
        in_specs=[anywhere] * (1 + n_small + 3) + [in_vmem] * 4 + [anywhere],
        out_specs=in_vmem,
        scratch_shapes=scratch,
        compiler_params=pltpu.CompilerParams(
            collective_id=0, has_side_effects=True, vmem_limit_bytes=62 * 1024 * 1024
        ),
    )
    return call, n_small


def solution(mesh):
    mesh_shape = dict(mesh.shape)

    def local(
        activations,
        norm_gain,
        query_weight,
        key_weight,
        value_weight,
        gate_weight,
        out_weight,
        mlp_gain,
        up_weight,
        down_weight,
    ):
        shapes = {
            "activations": activations.shape,
            "query_weight": query_weight.shape,
            "up_weight": up_weight.shape,
        }
        call, n_small = build(mesh_shape, shapes)
        small = (query_weight, key_weight, value_weight, gate_weight)
        if n_small == 1:
            small = (jnp.concatenate(small, axis=1),)
        cosine, sine, decay = tables(query_weight.shape[1])
        return call(
            activations,
            *small,
            out_weight,
            up_weight,
            down_weight,
            norm_gain.reshape(1, -1),
            mlp_gain.reshape(1, -1),
            jnp.asarray(cosine),
            jnp.asarray(sine),
            jnp.asarray(decay),
        )

    in_specs = (
        P(("rep", "fs"), "tp"),
        P(),
        P("fs", "tp"),
        P("fs", "tp"),
        P("fs", "tp"),
        P("fs", "tp"),
        P("tp", "fs"),
        P(),
        P("fs", "tp"),
        P("tp", "fs"),
    )
    return jax.shard_map(
        local, mesh=mesh, in_specs=in_specs, out_specs=P(("rep", "fs"), "tp"), check_vma=False
    )
```

```python
import functools

import jax
import jax.numpy as jnp
import numpy as np
from jax import lax
from jax.experimental import pallas as pl
from jax.experimental.pallas import tpu as pltpu
from jax.sharding import PartitionSpec as P

HEADS = 8
HEAD_DIM = 64
SEQ_LEN = 128
EPSILON = 1e-06
MESH = pl.DeviceIdType.MESH
BF16 = jnp.bfloat16
F32 = jnp.float32


def tables(head_width):
    half = HEAD_DIM // 2
    freqs = np.float32(10000.0) ** (-np.arange(half, dtype=np.float32) / np.float32(half))
    angle = np.arange(SEQ_LEN, dtype=np.float32)[:, None] * freqs[None, :]
    lane = np.arange(2 * head_width)
    scale = np.where(lane < head_width, 1.0, HEAD_DIM**-0.5).astype(np.float32)
    sign = np.where(lane % HEAD_DIM < half, -1.0, 1.0).astype(np.float32)
    cosine = np.cos(angle)[:, lane % half] * scale
    sine = np.sin(angle)[:, lane % half] * scale * sign
    exponent = np.float32(5.0) + np.float32(4.0) * np.arange(HEADS, dtype=np.float32) / np.float32(HEADS - 1)
    log_gamma = np.log(np.float32(1.0) - np.power(np.float32(2.0), -exponent))
    place = np.arange(SEQ_LEN, dtype=np.float32)
    distance = place[:, None] - place[None, :]
    decay = np.where(
        distance[None] >= 0,
        np.exp(np.maximum(distance, 0.0)[None] * log_gamma[:, None, None]),
        0.0,
    )
    return cosine.astype(np.float32), sine.astype(np.float32), decay.astype(np.float32)


NEAR_FOUR = {
    ("begin",): (
        ("alu", 0),
        ("ald", 3),
        ("ps", 2),
        ("acu", 1),
    ),
    ("act",): (
        ("acu", 0),
        ("ps", 1),
        ("ps", 3),
    ),
    ("proj", 1): (
        ("acd", 3),
        ("pu", 2, 1),
    ),
    ("proj", 2): (
        ("alu", 1),
    ),
    ("proj", 3): (
        ("ald", 2),
        ("pu", 1, 0),
        ("pu", 1, 1),
    ),
    ("mid",): (
        ("pu", 2, 0),
        ("acd", 2),
        ("acd", 1),
        ("pu", 3, 0),
        ("pu", 3, 1),
    ),
    ("m0",): (
        ("ald", 1),
    ),
    ("tok",): (
        ("pd", 2, 3),
        ("acd", 0),
        ("pd", 1, 2),
        ("pd", 1, 3),
        ("pd", 1, 1),
    ),
    ("m1",): (
        ("pd", 2, 2),
    ),
    ("raise", 0): (
        ("pd", 2, 1),
        ("pd", 2, 0),
        ("ald", 0),
    ),
    ("raise", 1): (
        ("pd", 1, 0),
    ),
    ("raise", 3): (
        ("pd", 3, 0),
        ("pd", 3, 1),
    ),
    ("low", 0, 0): (
        ("pd", 3, 2),
    ),
    ("low", 1, 0): (
        ("pd", 3, 3),
    ),
}
DEEP_FOUR = {
    ("begin",): (
        ("ald", 0),
        ("ald", 1),
        ("alu", 1),
        ("alu", 0),
        ("acu", 1),
        ("ald", 2),
        ("ald", 3),
        ("ps", 1),
        ("ps", 2),
    ),
    ("act",): (
        ("ps", 3),
    ),
    ("proj", 2): (
        ("acu", 0),
    ),
    ("proj", 3): (
        ("pu", 1, 1),
    ),
    ("ret",): (
        ("pd", 1, 2),
        ("pd", 1, 3),
        ("acd", 2),
        ("pu", 1, 0),
    ),
    ("mid",): (
        ("pu", 2, 0),
        ("pu", 2, 1),
    ),
    ("tok",): (
        ("acd", 3),
        ("pu", 3, 0),
        ("pu", 3, 1),
        ("acd", 0),
    ),
    ("m1",): (
        ("pd", 1, 1),
    ),
    ("raise", 0): (
        ("acd", 1),
        ("pd", 2, 3),
    ),
    ("raise", 1): (
        ("pd", 2, 2),
    ),
    ("low", 0, 0): (
        ("pd", 1, 0),
    ),
    ("low", 0, 1): (
        ("pd", 2, 0),
        ("pd", 2, 1),
    ),
    ("low", 1, 0): (
        ("pd", 3, 0),
    ),
    ("low", 2, 0): (
        ("pd", 3, 1),
    ),
    ("set", 0, 1): (
        ("pd", 3, 2),
    ),
    ("low", 2, 1): (
        ("pd", 3, 3),
    ),
}

DEEP_COLUMNS = (0, 2, 1, 3)


def spread_moves(planes):
    others = range(1, planes)
    return {
        ("begin",): tuple(("ps", k) for k in others) + (("alu", 0), ("acu", 0)),
        ("mid",): tuple(("pu", k, 0) for k in others) + (("ald", 0), ("acd", 0)),
        ("tok",): tuple(("pd", k, 0) for k in others),
    }


def chain(planes, units):
    steps = [("begin",), ("act",)] + [("proj", k) for k in range(1, planes)]
    steps += [("ret",), ("mid",), ("m0",), ("tok",), ("m1",)] + [("raise", k) for k in range(planes)]
    pieces = [(k, u) for k in range(planes) for u in range(units)]
    behind = 2 if units > 1 else 1
    for i, piece in enumerate(pieces):
        if i == len(pieces) - 1:
            steps.append(("left",))
        steps.append(("low", *piece))
        if i >= behind:
            steps.append(("set", *pieces[i - behind]))
    steps += [("set", *piece) for piece in pieces[-behind:]]
    return steps + [("end",)]


class Plan:
    def __init__(self):
        self.size = 0

    def take(self, count):
        base = self.size
        self.size += count
        return base


def build(mesh_shape, shapes):
    R, F, T = mesh_shape["rep"], mesh_shape["fs"], mesh_shape["tp"]
    X, HF, Q = T // 2, F // 2, F // T
    n, dc = shapes["activations"]
    dep, hw = shapes["query_weight"]
    fw = shapes["up_weight"][1]
    D = dc * T
    hid = fw // 2
    seqs = n // SEQ_LEN
    local_heads = hw // HEAD_DIM
    n_small = 4 if hw % 128 == 0 else 1
    sw = 4 * hw // n_small

    plan = Plan()
    L_ACT, L_OUT, L_UP, L_DOWN, L_DECAY, L_SMALL = (
        plan.take(1),
        plan.take(1),
        plan.take(1),
        plan.take(R),
        plan.take(1),
        plan.take(n_small),
    )

    class Spread:
        def __init__(self):
            self.send, self.recv = plan.take(2 * X - 1), plan.take(T)

    act_spread = Spread()
    ret_spread = [Spread() for _ in range(seqs)]
    mid_spread = [Spread() for _ in range(2)]
    mid_z = (plan.take(1), plan.take(1))
    om_send, om_recv = plan.take((T - 1) * Q), plan.take(T * Q)

    class Stream:
        def __init__(self, chunks, line):
            self.chunks, self.line = chunks, line
            self.zs, self.zf, self.zr = (plan.take(3 * chunks), plan.take(F * chunks), plan.take(F * chunks))
            self.ys, self.yr = plan.take(F * R * chunks), plan.take(F * R * chunks)

    near_moves, deep_moves = (NEAR_FOUR, DEEP_FOUR) if F == 4 else (spread_moves(F), spread_moves(F))
    up_chunks, down_chunks = (2, 4) if F == 4 else (1, 1)
    qkv_stream, out_stream = Stream(2, True), Stream(1, True)
    up_stream, down_stream = Stream(up_chunks, False), Stream(down_chunks, False)
    U = R if (dep // R) % 128 == 0 else 1
    uc = dep // U
    ps, pr = plan.take(2 * F * U), plan.take(2 * F * U)
    xs, xr = plan.take(2 * F * U), plan.take(2 * max(X - 1, 1) * Q * U)
    fz_s, fz_r = plan.take(Q * U), plan.take(Q * U)

    def kernel(*refs):
        act = refs[0]
        small = refs[1 : 1 + n_small]
        (out_w, up_w, down_w, gain1, gain2, cosine, sine, decay_all, result) = refs[1 + n_small : 10 + n_small]
        (
            act_full,
            normed,
            wbuf,
            proj,
            decay,
            og,
            om,
            ret,
            mid,
            second,
            upb,
            dnb,
            acc,
            hidden,
            pf,
            pbuf,
            srecv,
            tot,
            xrecv,
            zsnd,
            zrecv,
            sem,
        ) = refs[10 + n_small :]
        r, f, t = lax.axis_index("rep"), lax.axis_index("fs"), lax.axis_index("tp")
        x, c = t // 2, t % 2
        sib = 2 * x + 1 - c
        h = f // HF
        partner = (f + HF) % F

        def order(k):
            g = h * (F - 1 - f) + (1 - h) * f
            past = (k + 2 * F - 2 * g - 1) // (2 * F)
            odd = k % 2
            near = g + odd * ((k + 1) // 2) - (1 - odd) * (k // 2)
            s = past * k + (1 - past) * near
            return h * (F - 1 - s) + (1 - h) * s

        def at(i):
            return sem.at[i]

        def remote(src, dst, send, recv, **where):
            return pltpu.make_async_remote_copy(
                src_ref=src,
                dst_ref=dst,
                send_sem=at(send),
                recv_sem=at(recv),
                device_id=where,
                device_id_type=MESH,
            )

        def local(src, dst, i):
            return pltpu.make_async_copy(src, dst, at(i))

        def span(start, size, unit):
            return pl.ds(pl.multiple_of(start, unit), size)

        def act_block(s):
            return act_full.at[:, span(s * dc, dc, dc)]

        def mid_block(g, s):
            return mid.at[g, :, span(s * dc, dc, dc)]

        def ret_block(j, s):
            return ret.at[s, pl.ds(j * SEQ_LEN, SEQ_LEN), :]

        def rows_of(base, size, chunk, chunks):
            rows = size // chunks
            return span(base + chunk * rows, rows, rows)

        def qkv_part(s, part, ch):
            size = dep // R
            return wbuf.at[rows_of(s * dep + part * size, size, ch, qkv_stream.chunks), :]

        def out_part(s, part, ch):
            size = hw // R
            return og.at[s, rows_of(part * size, size, ch, out_stream.chunks), :]

        def up_part(s, part, ch):
            size = dep // R
            return upb.at[rows_of(s * dep + part * size, size, ch, up_stream.chunks), :]

        def down_part(s, part, ch):
            if U > 1:
                return dnb.at[s, part, rows_of(0, hid, ch, down_stream.chunks), :]
            size = hid // R
            return dnb.at[s, 0, rows_of(part * size, size, ch, down_stream.chunks), :]

        def qkv_own(half, ch):
            return qkv_part(f, r, ch)

        def out_own(half, ch):
            return out_part(f, r, ch)

        def up_own(half, ch):
            size = dep // R
            return up_w.at[rows_of(r * size, size, ch, up_stream.chunks), span(half * hid, hid, hid)]

        def down_own(half, ch):
            if U > 1:
                return down_w.at[rows_of(half * hid, hid, ch, down_stream.chunks), span(r * uc, uc, uc)]
            size = hid // R
            return down_w.at[rows_of(half * hid + r * size, size, ch, down_stream.chunks), :]

        def spread_copies(sp, block, source):
            first = [remote(source, block(t), sp.send, sp.recv + t, tp=sib)]
            for j in range(1, X):
                first.append(remote(source, block(t), sp.send + j, sp.recv + t, tp=((x + j) % X) * 2 + c))
            return first

        def spread_start(sp, block, source):
            for copy in reversed(spread_copies(sp, block, source)):
                copy.start()

        def relay_copy(sp, block, j):
            s = ((x + X - j) % X) * 2 + c
            return remote(block(s), block(s), sp.send + X - 1 + j, sp.recv + s, tp=sib)

        def spread_relay(sp, block):
            for j in range(1, X):
                s = ((x + X - j) % X) * 2 + c
                remote(block(s), block(s), sp.send, sp.recv + s, tp=sib).wait_recv()
                relay_copy(sp, block, j).start()

        def spread_finish(sp, block):
            for j in range(X):
                s = ((x + X - j) % X) * 2 + 1 - c
                remote(block(s), block(s), sp.send, sp.recv + s, tp=sib).wait_recv()

        def spread_drain(sp, block, source):
            for copy in spread_copies(sp, block, source):
                copy.wait_send()
            for j in range(1, X):
                relay_copy(sp, block, j).wait_send()

        deep = h * (f - HF) + (1 - h) * (HF - 1 - f)

        def y_copy(st, part, s, ch, q):
            block = part(s, r, ch)
            base = (s * R + q) * st.chunks + ch
            return remote(block, block, st.ys + base, st.yr + (s * R + r) * st.chunks + ch, rep=(r + q) % R)

        def y_wait(st, part, s):
            for q in range(1, R):
                other = (r + R - q) % R
                for ch in range(st.chunks):
                    block = part(s, other, ch)
                    remote(
                        block, block, st.ys, st.yr + (s * R + other) * st.chunks + ch, rep=other
                    ).wait_recv()

        def z_wait(st, part, s, ch):
            block = part(s, r, ch)
            remote(block, block, st.zs, st.zr + s * st.chunks + ch, fs=s).wait_recv()

        def along(st, part, own, what, chunks=None):
            size = F if st.line else HF
            for ch in range(st.chunks) if chunks is None else chunks:
                source, target, arrived = own(h, ch), part(f, r, ch), st.zr + f * st.chunks + ch

                @pl.when(f % size != size - 1)
                def _():
                    what(remote(source, target, st.zs + ch, arrived, fs=(f + 1) % F))

                @pl.when(f % size != 0)
                def _():
                    what(remote(source, target, st.zs + st.chunks + ch, arrived, fs=(f + F - 1) % F))

        def across(st, part, own, what, chunks=None):
            for ch in range(st.chunks) if chunks is None else chunks:
                what(
                    remote(
                        own(1 - h, ch),
                        part(f, r, ch),
                        st.zs + 2 * st.chunks + ch,
                        st.zr + f * st.chunks + ch,
                        fs=HF - h,
                    )
                )

        def forward(st, part, s, ch, what):
            after = f + 2 * ((f - s + F) // F) - 1
            size = F if st.line else HF

            @pl.when((after + size) // size - 1 == (0 if st.line else h))
            def _():
                block = part(s, r, ch)
                what(
                    remote(
                        block,
                        block,
                        st.zf + s * st.chunks + ch,
                        st.zr + s * st.chunks + ch,
                        fs=(after + F) % F,
                    )
                )

        def start(copy):
            copy.start()

        def leave(copy):
            copy.wait_send()

        def pass_on(st, part, k, chunks=None):
            s = order(k)
            for ch in range(st.chunks) if chunks is None else chunks:
                z_wait(st, part, s, ch)
                forward(st, part, s, ch, start)
                for q in range(1, R):
                    y_copy(st, part, s, ch, q).start()

        head0 = t * local_heads
        loads = [local(act, act_block(t), L_ACT)]
        for i in range(n_small):
            loads.append(local(small[i], wbuf.at[span(f * dep, dep, dep), pl.ds(i * sw, sw)], L_SMALL + i))
        loads.append(local(out_w, og.at[f], L_OUT))
        loads.append(local(decay_all.at[pl.ds(head0, local_heads)], decay, L_DECAY))
        loads.append(local(up_w.at[:, span(h * hid, hid, hid)], upb.at[span(f * dep, dep, dep), :], L_UP))
        for u in range(U):
            loads.append(
                local(down_w.at[span(h * hid, hid, hid), u * uc : (u + 1) * uc], dnb.at[f, u], L_DOWN + u)
            )
        for copy in loads:
            copy.start()

        barrier = pltpu.get_barrier_semaphore()
        for j in range(1, T):
            pl.semaphore_signal(barrier, inc=1, device_id={"tp": (t + j) % T}, device_id_type=MESH)
        for j in range(1, F):
            pl.semaphore_signal(barrier, inc=1, device_id={"fs": (f + j) % F}, device_id_type=MESH)
        for j in range(1, R):
            pl.semaphore_signal(barrier, inc=1, device_id={"rep": (r + j) % R}, device_id_type=MESH)
        pl.semaphore_wait(barrier, T + F + R - 3)

        def begin():
            spread_start(act_spread, act_block, act)
            for i in range(n_small):
                loads[1 + i].wait()
            along(qkv_stream, qkv_part, qkv_own, start)
            loads[1 + n_small].wait()
            along(out_stream, out_part, out_own, start)

        step = 64

        def norm_rows(source, gain, target):
            rows = source.astype(F32)
            mean = jnp.mean(rows * rows, axis=-1, keepdims=True)
            target[...] = (rows * lax.rsqrt(mean + EPSILON) * gain[...]).astype(BF16)

        def norm_first(i, carry):
            rows = span(i * step, step, step)
            norm_rows(act_full[rows, :], gain1, normed.at[rows, :])
            return carry

        def norm_act():
            loads[0].wait()
            spread_relay(act_spread, act_block)
            spread_finish(act_spread, act_block)
            lax.fori_loop(0, n // step, norm_first, 0)
            project(0)

        def project(k):
            s = order(k)
            part = jnp.dot(
                normed[:, span(s * dep, dep, dep)],
                wbuf[span(s * dep, dep, dep), :],
                preferred_element_type=F32,
            )
            if k == 0:
                proj[...] = part
            else:
                proj[...] += part

        def project_with(k):
            y_wait(qkv_stream, qkv_part, order(k))
            project(k)
            y_wait(out_stream, out_part, order(k))
            if k == F - 1:
                om_start()

        def om_copy(j, i):
            to = (t + j) % T
            return remote(
                og.at[to * Q + i],
                om.at[i, span(t * hw, hw, hw), :],
                om_send + (j - 1) * Q + i,
                om_recv + t * Q + i,
                tp=to,
            )

        def om_start():
            for j in range(1, T):
                for i in range(Q):
                    om_copy(j, i).start()
            for i in range(Q):
                om[i, span(t * hw, hw, hw), :] = og[t * Q + i]

        lane = lax.broadcasted_iota(jnp.int32, (SEQ_LEN, 2 * hw), 1)
        first_half = lane % HEAD_DIM < HEAD_DIM // 2
        head_of = lax.broadcasted_iota(jnp.int32, (SEQ_LEN, hw), 1) // HEAD_DIM

        def of_head(values, i):
            return values if local_heads == 1 else jnp.where(head_of == i, values, 0.0)

        def head_mean(values):
            total = jnp.zeros_like(values)
            for i in range(local_heads):
                mean = jnp.sum(of_head(values, i), axis=-1, keepdims=True) * (1.0 / HEAD_DIM)
                total += of_head(jnp.broadcast_to(mean, values.shape), i)
            return total

        def retain():
            loads[2 + n_small].wait()
            for j in range(seqs):
                rows = pl.ds(j * SEQ_LEN, SEQ_LEN)
                raw = proj[rows, : 2 * hw]
                turned = jnp.where(
                    first_half,
                    pltpu.roll(raw, 2 * hw - HEAD_DIM // 2, 1),
                    pltpu.roll(raw, HEAD_DIM // 2, 1),
                )
                both = raw * cosine[...] + turned * sine[...]
                query, key = both[:, :hw], both[:, hw:].astype(BF16)
                value = proj[rows, 2 * hw : 3 * hw]
                gate = proj[rows, 3 * hw :]
                mixed = jnp.zeros((SEQ_LEN, hw), F32)
                for i in range(local_heads):
                    scores = lax.dot_general(
                        of_head(query, i).astype(BF16), key, (((1,), (1,)), ((), ())), preferred_element_type=F32
                    )
                    weights = (scores * decay[i]).astype(BF16)
                    mixed += jnp.dot(weights, of_head(value, i).astype(BF16), preferred_element_type=F32)
                centred = mixed - head_mean(mixed)
                spread_of = lax.rsqrt(head_mean(centred * centred) + EPSILON)
                ret[t, rows, :] = (centred * spread_of * (gate * jax.nn.sigmoid(gate))).astype(BF16)
                block = functools.partial(ret_block, j)
                spread_start(ret_spread[j], block, block(t))

        mid_own = functools.partial(mid_block, 0)
        mid_other = functools.partial(mid_block, 1)
        to_partner = remote(mid_own(t), mid_other(t), mid_z[0], mid_z[1], fs=partner)

        def middle():
            for j in range(1, T):
                s = (t + T - j) % T
                for i in range(Q):
                    block = om.at[i, span(s * hw, hw, hw), :]
                    remote(block, block, om_send, om_recv + s * Q + i, tp=s).wait_recv()
            for j in range(seqs):
                spread_relay(ret_spread[j], functools.partial(ret_block, j))
            for j in range(seqs):
                block = functools.partial(ret_block, j)
                spread_finish(ret_spread[j], block)
                rows = pl.ds(j * SEQ_LEN, SEQ_LEN)
                for i in range(Q):
                    branch = jnp.zeros((SEQ_LEN, dep), F32)
                    for s in range(T):
                        branch += jnp.dot(
                            ret[s, rows, :], om[i, pl.ds(s * hw, hw), :], preferred_element_type=F32
                        )
                    columns = span(t * dc + i * dep, dep, dep)
                    mid[0, rows, columns] = (act_full[rows, columns].astype(F32) + branch).astype(BF16)
            spread_start(mid_spread[0], mid_own, mid_own(t))
            to_partner.start()

        def norm_second(g):
            def body(i, carry):
                rows = span(i * step, step, step)
                norm_rows(mid[g, rows, :], gain2, second.at[g, rows, :])
                return carry

            block = mid_other if g else mid_own
            spread_relay(mid_spread[g], block)
            spread_finish(mid_spread[g], block)
            lax.fori_loop(0, n // step, body, 0)

        def partner_rows():
            to_partner.wait_recv()
            spread_start(mid_spread[1], mid_other, mid_other(t))

        def raise_by(k):
            s = order(k)
            if k == 0:
                loads[3 + n_small].wait()
            else:
                y_wait(up_stream, up_part, s)
            for g in range(2):
                part = jnp.dot(
                    second[g, :, span(s * dep, dep, dep)],
                    upb[span(s * dep, dep, dep), :],
                    preferred_element_type=F32,
                )
                if k == 0:
                    acc[g] = part
                elif k < F - 1:
                    acc[g] += part
                else:
                    kept = jnp.maximum(acc[g] + part, 0.0)
                    hidden[g] = (kept * kept).astype(BF16)

        def p_copy(s, u, g):
            i = (s * U + u) * 2 + g
            return remote(pbuf.at[s, u, g], srecv.at[s, u, g], ps + i, pr + i, tp=sib)

        def x_copy(s, u, g):
            td, i = s // Q, s % Q
            away = (x + X - td // 2) % X
            slot = (away + X - 1) % X % max(X - 1, 1)
            return remote(
                pbuf.at[s, u, g],
                xrecv.at[slot, g, i, u],
                xs + (s * U + u) * 2 + g,
                xr + ((slot * 2 + g) * Q + i) * U + u,
                tp=(td // 2) * 2 + c,
            )

        def z_copy(i, u):
            return remote(zsnd.at[i, u], zrecv.at[i, u], fz_s + i * U + u, fz_r + i * U + u, fs=partner)

        def unit(u):
            return (r + u) % U

        def low_order(k):
            if F != 4:
                return order(k)
            return (1 - deep) * order(k) + deep * order(DEEP_COLUMNS[k])

        def lower(k, u):
            s = low_order(k)
            if k == 0 and u == 0:
                for copy in loads[4 + n_small :]:
                    copy.wait()
            if k > 0 and u == U - 1:
                y_wait(down_stream, down_part, s)
            u = unit(u)
            td, i = s // Q, s % Q
            xd, cd = td // 2, td % 2
            for g in (1, 0):
                pf[g] = jnp.dot(hidden[g], dnb[s, u], preferred_element_type=F32)

                @pl.when(c != cd)
                def _():
                    pbuf[s, u, g] = pf[g].astype(BF16)
                    p_copy(s, u, g).start()

            @pl.when(c == cd)
            def _():
                for g in (1, 0):
                    p_copy(s, u, g).wait_recv()
                    total = pf[g] + srecv[s, u, g].astype(F32)

                    @pl.when(x == xd)
                    def _():
                        tot[g, i, u] = total

                    @pl.when(x != xd)
                    def _():
                        pbuf[s, u, g] = total.astype(BF16)
                        x_copy(s, u, g).start()

        def settle(k, u):
            s = low_order(k)
            u = unit(u)
            td, i = s // Q, s % Q

            @pl.when(td == t)
            def _():
                for g in (1, 0):
                    total = tot[g, i, u]
                    for slot in range(X - 1):
                        block = xrecv.at[slot, g, i, u]
                        remote(block, block, xs, xr + ((slot * 2 + g) * Q + i) * U + u, tp=sib).wait_recv()
                        total += xrecv[slot, g, i, u].astype(F32)
                    if g == 1:
                        zsnd[i, u] = total.astype(BF16)
                        z_copy(i, u).start()
                    else:
                        tot[0, i, u] = total

        def finish():
            for i in range(Q):
                for u in range(U):
                    z_copy(i, u).wait_recv()
                    base = i * dep + u * uc
                    columns = span(t * dc + base, uc, uc)
                    result[:, base : base + uc] = (
                        mid[0, :, columns].astype(F32) + (tot[0, i, u] + zrecv[i, u].astype(F32))
                    ).astype(BF16)

        streams = (
            (qkv_stream, qkv_part, qkv_own),
            (out_stream, out_part, out_own),
            (up_stream, up_part, up_own),
            (down_stream, down_part, down_own),
        )

        def passed(st, part, k):
            s = order(k)
            for ch in range(st.chunks):
                forward(st, part, s, ch, leave)
                for q in range(1, R):
                    y_copy(st, part, s, ch, q).wait_send()

        def summed(k):
            s = low_order(k)
            td = s // Q
            for u in range(U):
                for g in range(2):

                    @pl.when(c != td % 2)
                    def _():
                        p_copy(s, u, g).wait_send()

                    @pl.when((c == td % 2) & (x != td // 2))
                    def _():
                        x_copy(s, u, g).wait_send()

        def early_left():
            spread_drain(act_spread, act_block, act)
            for j in range(seqs):
                block = functools.partial(ret_block, j)
                spread_drain(ret_spread[j], block, block(t))
            spread_drain(mid_spread[0], mid_own, mid_own(t))
            spread_drain(mid_spread[1], mid_other, mid_other(t))
            to_partner.wait_send()
            for j in range(1, T):
                for i in range(Q):
                    om_copy(j, i).wait_send()
            for st, part, own in streams:
                along(st, part, own, leave)
                if not st.line:
                    across(st, part, own, leave)

            def sent(k, carry):
                for st, part, own in streams[:3]:
                    passed(st, part, k)
                return carry

            def sent_down(k, carry):
                passed(down_stream, down_part, k)
                return carry

            lax.fori_loop(1, F, sent, 0)
            lax.fori_loop(1, F - 1, sent_down, 0)
            for k in range(F - 2):
                summed(k)

        def late_left():
            passed(down_stream, down_part, F - 1)
            for k in range(F - 2, F):
                summed(k)
            for i in range(Q):
                for u in range(U):
                    z_copy(i, u).wait_send()

        near = deep == 0
        steps = {
            "begin": begin,
            "act": norm_act,
            "proj": project_with,
            "ret": retain,
            "mid": middle,
            "m0": lambda: norm_second(0),
            "tok": partner_rows,
            "m1": lambda: norm_second(1),
            "raise": raise_by,
            "low": lower,
            "set": settle,
            "left": early_left,
            "end": finish,
        }

        def small_on(k):
            pass_on(qkv_stream, qkv_part, k)
            pass_on(out_stream, out_part, k)

        moves = {
            "ps": small_on,
            "alu": lambda ch: along(up_stream, up_part, up_own, start, (ch,)),
            "acu": lambda ch: across(up_stream, up_part, up_own, start, (ch,)),
            "ald": lambda ch: along(down_stream, down_part, down_own, start, (ch,)),
            "acd": lambda ch: across(down_stream, down_part, down_own, start, (ch,)),
            "pu": lambda k, ch: pass_on(up_stream, up_part, k, (ch,)),
            "pd": lambda k, ch: pass_on(down_stream, down_part, k, (ch,)),
        }
        for name, *place in chain(F, U):
            steps[name](*place)
            for here, table in ((near, near_moves), (deep > 0, deep_moves)):
                todo = table.get((name, *place), ())
                if todo:

                    @pl.when(here)
                    def _():
                        for move, *which in todo:
                            moves[move](*which)

        late_left()

    vmem = pltpu.VMEM
    scratch = [
        vmem((n, D), BF16),
        vmem((n, D), BF16),
        vmem((D, 4 * hw), BF16),
        vmem((n, 4 * hw), F32),
        vmem((local_heads, SEQ_LEN, SEQ_LEN), F32),
        vmem((F, hw, dep), BF16),
        vmem((Q, T * hw, dep), BF16),
        vmem((T, n, hw), BF16),
        vmem((2, n, D), BF16),
        vmem((2, n, D), BF16),
        vmem((D, hid), BF16),
        vmem((F, U, hid, uc), BF16),
        vmem((2, n, hid), F32),
        vmem((2, n, hid), BF16),
        vmem((2, n, uc), F32),
        vmem((F, U, 2, n, uc), BF16),
        vmem((F, U, 2, n, uc), BF16),
        vmem((2, Q, U, n, uc), F32),
        vmem((max(X - 1, 1), 2, Q, U, n, uc), BF16),
        vmem((Q, U, n, uc), BF16),
        vmem((Q, U, n, uc), BF16),
        pltpu.SemaphoreType.DMA((plan.size,)),
    ]
    anywhere = pl.BlockSpec(memory_space=pl.ANY)
    in_vmem = pl.BlockSpec(memory_space=vmem)
    call = pl.pallas_call(
        kernel,
        name="layer",
        out_shape=jax.ShapeDtypeStruct((n, dc), BF16),
        in_specs=[anywhere] * (1 + n_small + 3) + [in_vmem] * 4 + [anywhere],
        out_specs=in_vmem,
        scratch_shapes=scratch,
        compiler_params=pltpu.CompilerParams(
            collective_id=0, has_side_effects=True, vmem_limit_bytes=62 * 1024 * 1024
        ),
    )
    return call, n_small


def solution(mesh):
    mesh_shape = dict(mesh.shape)

    def local(
        activations,
        norm_gain,
        query_weight,
        key_weight,
        value_weight,
        gate_weight,
        out_weight,
        mlp_gain,
        up_weight,
        down_weight,
    ):
        shapes = {
            "activations": activations.shape,
            "query_weight": query_weight.shape,
            "up_weight": up_weight.shape,
        }
        call, n_small = build(mesh_shape, shapes)
        small = (query_weight, key_weight, value_weight, gate_weight)
        if n_small == 1:
            small = (jnp.concatenate(small, axis=1),)
        cosine, sine, decay = tables(query_weight.shape[1])
        return call(
            activations,
            *small,
            out_weight,
            up_weight,
            down_weight,
            norm_gain.reshape(1, -1),
            mlp_gain.reshape(1, -1),
            jnp.asarray(cosine),
            jnp.asarray(sine),
            jnp.asarray(decay),
        )

    in_specs = (
        P(("rep", "fs"), "tp"),
        P(),
        P("fs", "tp"),
        P("fs", "tp"),
        P("fs", "tp"),
        P("fs", "tp"),
        P("tp", "fs"),
        P(),
        P("fs", "tp"),
        P("tp", "fs"),
    )
    return jax.shard_map(
        local, mesh=mesh, in_specs=in_specs, out_specs=P(("rep", "fs"), "tp"), check_vma=False
    )
```

```python
import functools

import jax
import jax.numpy as jnp
import numpy as np
from jax import lax
from jax.experimental import pallas as pl
from jax.experimental.pallas import tpu as pltpu
from jax.sharding import PartitionSpec as P

HEADS = 8
HEAD_DIM = 64
SEQ_LEN = 128
EPSILON = 1e-06
MESH = pl.DeviceIdType.MESH
BF16 = jnp.bfloat16
F32 = jnp.float32


def tables(head_width):
    half = HEAD_DIM // 2
    freqs = np.float32(10000.0) ** (-np.arange(half, dtype=np.float32) / np.float32(half))
    angle = np.arange(SEQ_LEN, dtype=np.float32)[:, None] * freqs[None, :]
    lane = np.arange(2 * head_width)
    scale = np.where(lane < head_width, 1.0, HEAD_DIM**-0.5).astype(np.float32)
    sign = np.where(lane % HEAD_DIM < half, -1.0, 1.0).astype(np.float32)
    cosine = np.cos(angle)[:, lane % half] * scale
    sine = np.sin(angle)[:, lane % half] * scale * sign
    exponent = np.float32(5.0) + np.float32(4.0) * np.arange(HEADS, dtype=np.float32) / np.float32(HEADS - 1)
    log_gamma = np.log(np.float32(1.0) - np.power(np.float32(2.0), -exponent))
    place = np.arange(SEQ_LEN, dtype=np.float32)
    distance = place[:, None] - place[None, :]
    decay = np.where(
        distance[None] >= 0,
        np.exp(np.maximum(distance, 0.0)[None] * log_gamma[:, None, None]),
        0.0,
    )
    return cosine.astype(np.float32), sine.astype(np.float32), decay.astype(np.float32)


NEAR_FOUR = {
    ("begin",): (
        ("alu", 0),
        ("ald", 3),
        ("ps", 2),
        ("acu", 1),
    ),
    ("act",): (
        ("acu", 0),
        ("ps", 1),
        ("ps", 3),
    ),
    ("proj", 1): (
        ("acd", 3),
        ("pu", 2, 1),
    ),
    ("proj", 2): (
        ("alu", 1),
    ),
    ("proj", 3): (
        ("ald", 2),
        ("pu", 1, 0),
        ("pu", 1, 1),
    ),
    ("mid",): (
        ("pu", 2, 0),
        ("acd", 2),
        ("acd", 1),
        ("pu", 3, 0),
        ("pu", 3, 1),
    ),
    ("m0",): (
        ("ald", 1),
    ),
    ("tok",): (
        ("pd", 2, 3),
        ("acd", 0),
        ("pd", 1, 2),
        ("pd", 1, 3),
        ("pd", 1, 1),
    ),
    ("m1",): (
        ("pd", 2, 2),
    ),
    ("raise", 0): (
        ("pd", 2, 1),
        ("pd", 2, 0),
        ("ald", 0),
    ),
    ("raise", 1): (
        ("pd", 1, 0),
    ),
    ("raise", 3): (
        ("pd", 3, 0),
        ("pd", 3, 1),
    ),
    ("low", 0, 0): (
        ("pd", 3, 2),
    ),
    ("low", 1, 0): (
        ("pd", 3, 3),
    ),
}
DEEP_FOUR = {
    ("begin",): (
        ("ald", 0),
        ("ald", 1),
        ("alu", 1),
        ("alu", 0),
        ("acu", 1),
        ("ald", 2),
        ("ald", 3),
        ("ps", 1),
        ("ps", 2),
    ),
    ("act",): (
        ("ps", 3),
    ),
    ("proj", 2): (
        ("acu", 0),
    ),
    ("proj", 3): (
        ("pu", 1, 1),
    ),
    ("ret",): (
        ("pd", 1, 2),
        ("pd", 1, 3),
        ("acd", 2),
        ("pu", 1, 0),
    ),
    ("mid",): (
        ("pu", 2, 0),
        ("pu", 2, 1),
    ),
    ("tok",): (
        ("acd", 3),
        ("pu", 3, 0),
        ("pu", 3, 1),
        ("acd", 0),
    ),
    ("m1",): (
        ("pd", 1, 1),
    ),
    ("raise", 0): (
        ("acd", 1),
        ("pd", 2, 3),
    ),
    ("raise", 1): (
        ("pd", 2, 2),
    ),
    ("low", 0, 0): (
        ("pd", 1, 0),
    ),
    ("low", 0, 1): (
        ("pd", 2, 0),
        ("pd", 2, 1),
    ),
    ("low", 1, 0): (
        ("pd", 3, 0),
    ),
    ("low", 2, 0): (
        ("pd", 3, 2),
    ),
    ("set", 0, 1): (
        ("pd", 3, 1),
    ),
    ("low", 2, 1): (
        ("pd", 3, 3),
    ),
}

DEEP_COLUMNS = (0, 2, 1, 3)


def spread_moves(planes):
    others = range(1, planes)
    return {
        ("begin",): tuple(("ps", k) for k in others) + (("alu", 0), ("acu", 0)),
        ("mid",): tuple(("pu", k, 0) for k in others) + (("ald", 0), ("acd", 0)),
        ("tok",): tuple(("pd", k, 0) for k in others),
    }


def chain(planes, units):
    steps = [("begin",), ("act",)] + [("proj", k) for k in range(1, planes)]
    steps += [("ret",), ("mid",), ("m0",), ("tok",), ("m1",)] + [("raise", k) for k in range(planes)]
    pieces = [(k, u) for k in range(planes) for u in range(units)]
    behind = 2 if units > 1 else 1
    for i, piece in enumerate(pieces):
        if i == len(pieces) - 1:
            steps.append(("left",))
        steps.append(("low", *piece))
        if i >= behind:
            steps.append(("set", *pieces[i - behind]))
    steps += [("set", *piece) for piece in pieces[-behind:]]
    return steps + [("end",)]


class Plan:
    def __init__(self):
        self.size = 0

    def take(self, count):
        base = self.size
        self.size += count
        return base


def build(mesh_shape, shapes):
    R, F, T = mesh_shape["rep"], mesh_shape["fs"], mesh_shape["tp"]
    X, HF, Q = T // 2, F // 2, F // T
    n, dc = shapes["activations"]
    dep, hw = shapes["query_weight"]
    fw = shapes["up_weight"][1]
    D = dc * T
    hid = fw // 2
    seqs = n // SEQ_LEN
    local_heads = hw // HEAD_DIM
    n_small = 4 if hw % 128 == 0 else 1
    sw = 4 * hw // n_small

    plan = Plan()
    L_ACT, L_OUT, L_UP, L_DOWN, L_DECAY, L_SMALL = (
        plan.take(1),
        plan.take(1),
        plan.take(1),
        plan.take(R),
        plan.take(1),
        plan.take(n_small),
    )

    class Spread:
        def __init__(self):
            self.send, self.recv = plan.take(2 * X - 1), plan.take(T)

    act_spread = Spread()
    ret_spread = [Spread() for _ in range(seqs)]
    mid_spread = [Spread() for _ in range(2)]
    mid_z = (plan.take(1), plan.take(1))
    om_send, om_recv = plan.take((T - 1) * Q), plan.take(T * Q)

    class Stream:
        def __init__(self, chunks, line):
            self.chunks, self.line = chunks, line
            self.zs, self.zf, self.zr = (plan.take(3 * chunks), plan.take(F * chunks), plan.take(F * chunks))
            self.ys, self.yr = plan.take(F * R * chunks), plan.take(F * R * chunks)

    near_moves, deep_moves = (NEAR_FOUR, DEEP_FOUR) if F == 4 else (spread_moves(F), spread_moves(F))
    up_chunks, down_chunks = (2, 4) if F == 4 else (1, 1)
    qkv_stream, out_stream = Stream(2, True), Stream(1, True)
    up_stream, down_stream = Stream(up_chunks, False), Stream(down_chunks, False)
    U = R if (dep // R) % 128 == 0 else 1
    uc = dep // U
    ps, pr = plan.take(2 * F * U), plan.take(2 * F * U)
    xs, xr = plan.take(2 * F * U), plan.take(2 * max(X - 1, 1) * Q * U)
    fz_s, fz_r = plan.take(Q * U), plan.take(Q * U)

    def kernel(*refs):
        act = refs[0]
        small = refs[1 : 1 + n_small]
        (out_w, up_w, down_w, gain1, gain2, cosine, sine, decay_all, result) = refs[1 + n_small : 10 + n_small]
        (
            act_full,
            normed,
            wbuf,
            proj,
            decay,
            og,
            om,
            ret,
            mid,
            second,
            upb,
            dnb,
            acc,
            hidden,
            pf,
            pbuf,
            srecv,
            tot,
            xrecv,
            zsnd,
            zrecv,
            sem,
        ) = refs[10 + n_small :]
        r, f, t = lax.axis_index("rep"), lax.axis_index("fs"), lax.axis_index("tp")
        x, c = t // 2, t % 2
        sib = 2 * x + 1 - c
        h = f // HF
        partner = (f + HF) % F

        def order(k):
            g = h * (F - 1 - f) + (1 - h) * f
            past = (k + 2 * F - 2 * g - 1) // (2 * F)
            odd = k % 2
            near = g + odd * ((k + 1) // 2) - (1 - odd) * (k // 2)
            s = past * k + (1 - past) * near
            return h * (F - 1 - s) + (1 - h) * s

        def at(i):
            return sem.at[i]

        def remote(src, dst, send, recv, **where):
            return pltpu.make_async_remote_copy(
                src_ref=src,
                dst_ref=dst,
                send_sem=at(send),
                recv_sem=at(recv),
                device_id=where,
                device_id_type=MESH,
            )

        def local(src, dst, i):
            return pltpu.make_async_copy(src, dst, at(i))

        def span(start, size, unit):
            return pl.ds(pl.multiple_of(start, unit), size)

        def act_block(s):
            return act_full.at[:, span(s * dc, dc, dc)]

        def mid_block(g, s):
            return mid.at[g, :, span(s * dc, dc, dc)]

        def ret_block(j, s):
            return ret.at[s, pl.ds(j * SEQ_LEN, SEQ_LEN), :]

        def rows_of(base, size, chunk, chunks):
            rows = size // chunks
            return span(base + chunk * rows, rows, rows)

        def qkv_part(s, part, ch):
            size = dep // R
            return wbuf.at[rows_of(s * dep + part * size, size, ch, qkv_stream.chunks), :]

        def out_part(s, part, ch):
            size = hw // R
            return og.at[s, rows_of(part * size, size, ch, out_stream.chunks), :]

        def up_part(s, part, ch):
            size = dep // R
            return upb.at[rows_of(s * dep + part * size, size, ch, up_stream.chunks), :]

        def down_part(s, part, ch):
            if U > 1:
                return dnb.at[s, part, rows_of(0, hid, ch, down_stream.chunks), :]
            size = hid // R
            return dnb.at[s, 0, rows_of(part * size, size, ch, down_stream.chunks), :]

        def qkv_own(half, ch):
            return qkv_part(f, r, ch)

        def out_own(half, ch):
            return out_part(f, r, ch)

        def up_own(half, ch):
            size = dep // R
            return up_w.at[rows_of(r * size, size, ch, up_stream.chunks), span(half * hid, hid, hid)]

        def down_own(half, ch):
            if U > 1:
                return down_w.at[rows_of(half * hid, hid, ch, down_stream.chunks), span(r * uc, uc, uc)]
            size = hid // R
            return down_w.at[rows_of(half * hid + r * size, size, ch, down_stream.chunks), :]

        def spread_copies(sp, block, source):
            first = [remote(source, block(t), sp.send, sp.recv + t, tp=sib)]
            for j in range(1, X):
                first.append(remote(source, block(t), sp.send + j, sp.recv + t, tp=((x + j) % X) * 2 + c))
            return first

        def spread_start(sp, block, source):
            for copy in reversed(spread_copies(sp, block, source)):
                copy.start()

        def relay_copy(sp, block, j):
            s = ((x + X - j) % X) * 2 + c
            return remote(block(s), block(s), sp.send + X - 1 + j, sp.recv + s, tp=sib)

        def spread_relay(sp, block):
            for j in range(1, X):
                s = ((x + X - j) % X) * 2 + c
                remote(block(s), block(s), sp.send, sp.recv + s, tp=sib).wait_recv()
                relay_copy(sp, block, j).start()

        def spread_finish(sp, block):
            for j in range(X):
                s = ((x + X - j) % X) * 2 + 1 - c
                remote(block(s), block(s), sp.send, sp.recv + s, tp=sib).wait_recv()

        def spread_drain(sp, block, source):
            for copy in spread_copies(sp, block, source):
                copy.wait_send()
            for j in range(1, X):
                relay_copy(sp, block, j).wait_send()

        deep = h * (f - HF) + (1 - h) * (HF - 1 - f)

        def y_copy(st, part, s, ch, q):
            block = part(s, r, ch)
            base = (s * R + q) * st.chunks + ch
            return remote(block, block, st.ys + base, st.yr + (s * R + r) * st.chunks + ch, rep=(r + q) % R)

        def y_wait(st, part, s):
            for q in range(1, R):
                other = (r + R - q) % R
                for ch in range(st.chunks):
                    block = part(s, other, ch)
                    remote(
                        block, block, st.ys, st.yr + (s * R + other) * st.chunks + ch, rep=other
                    ).wait_recv()

        def z_wait(st, part, s, ch):
            block = part(s, r, ch)
            remote(block, block, st.zs, st.zr + s * st.chunks + ch, fs=s).wait_recv()

        def along(st, part, own, what, chunks=None):
            size = F if st.line else HF
            for ch in range(st.chunks) if chunks is None else chunks:
                source, target, arrived = own(h, ch), part(f, r, ch), st.zr + f * st.chunks + ch

                @pl.when(f % size != size - 1)
                def _():
                    what(remote(source, target, st.zs + ch, arrived, fs=(f + 1) % F))

                @pl.when(f % size != 0)
                def _():
                    what(remote(source, target, st.zs + st.chunks + ch, arrived, fs=(f + F - 1) % F))

        def across(st, part, own, what, chunks=None):
            for ch in range(st.chunks) if chunks is None else chunks:
                what(
                    remote(
                        own(1 - h, ch),
                        part(f, r, ch),
                        st.zs + 2 * st.chunks + ch,
                        st.zr + f * st.chunks + ch,
                        fs=HF - h,
                    )
                )

        def forward(st, part, s, ch, what):
            after = f + 2 * ((f - s + F) // F) - 1
            size = F if st.line else HF

            @pl.when((after + size) // size - 1 == (0 if st.line else h))
            def _():
                block = part(s, r, ch)
                what(
                    remote(
                        block,
                        block,
                        st.zf + s * st.chunks + ch,
                        st.zr + s * st.chunks + ch,
                        fs=(after + F) % F,
                    )
                )

        def start(copy):
            copy.start()

        def leave(copy):
            copy.wait_send()

        def pass_on(st, part, k, chunks=None):
            s = order(k)
            for ch in range(st.chunks) if chunks is None else chunks:
                z_wait(st, part, s, ch)
                forward(st, part, s, ch, start)
                for q in range(1, R):
                    y_copy(st, part, s, ch, q).start()

        head0 = t * local_heads
        loads = [local(act, act_block(t), L_ACT)]
        for i in range(n_small):
            loads.append(local(small[i], wbuf.at[span(f * dep, dep, dep), pl.ds(i * sw, sw)], L_SMALL + i))
        loads.append(local(out_w, og.at[f], L_OUT))
        loads.append(local(decay_all.at[pl.ds(head0, local_heads)], decay, L_DECAY))
        loads.append(local(up_w.at[:, span(h * hid, hid, hid)], upb.at[span(f * dep, dep, dep), :], L_UP))
        for u in range(U):
            loads.append(
                local(down_w.at[span(h * hid, hid, hid), u * uc : (u + 1) * uc], dnb.at[f, u], L_DOWN + u)
            )
        for copy in loads:
            copy.start()

        barrier = pltpu.get_barrier_semaphore()
        for j in range(1, T):
            pl.semaphore_signal(barrier, inc=1, device_id={"tp": (t + j) % T}, device_id_type=MESH)
        for j in range(1, F):
            pl.semaphore_signal(barrier, inc=1, device_id={"fs": (f + j) % F}, device_id_type=MESH)
        for j in range(1, R):
            pl.semaphore_signal(barrier, inc=1, device_id={"rep": (r + j) % R}, device_id_type=MESH)
        pl.semaphore_wait(barrier, T + F + R - 3)

        def begin():
            spread_start(act_spread, act_block, act)
            for i in range(n_small):
                loads[1 + i].wait()
            along(qkv_stream, qkv_part, qkv_own, start)
            loads[1 + n_small].wait()
            along(out_stream, out_part, out_own, start)

        step = 64

        def norm_rows(source, gain, target):
            rows = source.astype(F32)
            mean = jnp.mean(rows * rows, axis=-1, keepdims=True)
            target[...] = (rows * lax.rsqrt(mean + EPSILON) * gain[...]).astype(BF16)

        def norm_first(i, carry):
            rows = span(i * step, step, step)
            norm_rows(act_full[rows, :], gain1, normed.at[rows, :])
            return carry

        def norm_act():
            loads[0].wait()
            spread_relay(act_spread, act_block)
            spread_finish(act_spread, act_block)
            lax.fori_loop(0, n // step, norm_first, 0)
            project(0)

        def project(k):
            s = order(k)
            part = jnp.dot(
                normed[:, span(s * dep, dep, dep)],
                wbuf[span(s * dep, dep, dep), :],
                preferred_element_type=F32,
            )
            if k == 0:
                proj[...] = part
            else:
                proj[...] += part

        def project_with(k):
            y_wait(qkv_stream, qkv_part, order(k))
            project(k)
            y_wait(out_stream, out_part, order(k))
            if k == F - 1:
                om_start()

        def om_copy(j, i):
            to = (t + j) % T
            return remote(
                og.at[to * Q + i],
                om.at[i, span(t * hw, hw, hw), :],
                om_send + (j - 1) * Q + i,
                om_recv + t * Q + i,
                tp=to,
            )

        def om_start():
            for j in range(1, T):
                for i in range(Q):
                    om_copy(j, i).start()
            for i in range(Q):
                om[i, span(t * hw, hw, hw), :] = og[t * Q + i]

        lane = lax.broadcasted_iota(jnp.int32, (SEQ_LEN, 2 * hw), 1)
        first_half = lane % HEAD_DIM < HEAD_DIM // 2
        head_of = lax.broadcasted_iota(jnp.int32, (SEQ_LEN, hw), 1) // HEAD_DIM

        def of_head(values, i):
            return values if local_heads == 1 else jnp.where(head_of == i, values, 0.0)

        def head_mean(values):
            total = jnp.zeros_like(values)
            for i in range(local_heads):
                mean = jnp.sum(of_head(values, i), axis=-1, keepdims=True) * (1.0 / HEAD_DIM)
                total += of_head(jnp.broadcast_to(mean, values.shape), i)
            return total

        def retain():
            loads[2 + n_small].wait()
            for j in range(seqs):
                rows = pl.ds(j * SEQ_LEN, SEQ_LEN)
                raw = proj[rows, : 2 * hw]
                turned = jnp.where(
                    first_half,
                    pltpu.roll(raw, 2 * hw - HEAD_DIM // 2, 1),
                    pltpu.roll(raw, HEAD_DIM // 2, 1),
                )
                both = raw * cosine[...] + turned * sine[...]
                query, key = both[:, :hw], both[:, hw:].astype(BF16)
                value = proj[rows, 2 * hw : 3 * hw]
                gate = proj[rows, 3 * hw :]
                mixed = jnp.zeros((SEQ_LEN, hw), F32)
                for i in range(local_heads):
                    scores = lax.dot_general(
                        of_head(query, i).astype(BF16), key, (((1,), (1,)), ((), ())), preferred_element_type=F32
                    )
                    weights = (scores * decay[i]).astype(BF16)
                    mixed += jnp.dot(weights, of_head(value, i).astype(BF16), preferred_element_type=F32)
                centred = mixed - head_mean(mixed)
                spread_of = lax.rsqrt(head_mean(centred * centred) + EPSILON)
                ret[t, rows, :] = (centred * spread_of * (gate * jax.nn.sigmoid(gate))).astype(BF16)
                block = functools.partial(ret_block, j)
                spread_start(ret_spread[j], block, block(t))

        mid_own = functools.partial(mid_block, 0)
        mid_other = functools.partial(mid_block, 1)
        to_partner = remote(mid_own(t), mid_other(t), mid_z[0], mid_z[1], fs=partner)

        def middle():
            for j in range(1, T):
                s = (t + T - j) % T
                for i in range(Q):
                    block = om.at[i, span(s * hw, hw, hw), :]
                    remote(block, block, om_send, om_recv + s * Q + i, tp=s).wait_recv()
            for j in range(seqs):
                spread_relay(ret_spread[j], functools.partial(ret_block, j))
            for j in range(seqs):
                block = functools.partial(ret_block, j)
                spread_finish(ret_spread[j], block)
                rows = pl.ds(j * SEQ_LEN, SEQ_LEN)
                for i in range(Q):
                    branch = jnp.zeros((SEQ_LEN, dep), F32)
                    for s in range(T):
                        branch += jnp.dot(
                            ret[s, rows, :], om[i, pl.ds(s * hw, hw), :], preferred_element_type=F32
                        )
                    columns = span(t * dc + i * dep, dep, dep)
                    mid[0, rows, columns] = (act_full[rows, columns].astype(F32) + branch).astype(BF16)
            spread_start(mid_spread[0], mid_own, mid_own(t))
            to_partner.start()

        def norm_second(g):
            def body(i, carry):
                rows = span(i * step, step, step)
                norm_rows(mid[g, rows, :], gain2, second.at[g, rows, :])
                return carry

            block = mid_other if g else mid_own
            spread_relay(mid_spread[g], block)
            spread_finish(mid_spread[g], block)
            lax.fori_loop(0, n // step, body, 0)

        def partner_rows():
            to_partner.wait_recv()
            spread_start(mid_spread[1], mid_other, mid_other(t))

        def raise_by(k):
            s = order(k)
            if k == 0:
                loads[3 + n_small].wait()
            else:
                y_wait(up_stream, up_part, s)
            for g in range(2):
                part = jnp.dot(
                    second[g, :, span(s * dep, dep, dep)],
                    upb[span(s * dep, dep, dep), :],
                    preferred_element_type=F32,
                )
                if k == 0:
                    acc[g] = part
                elif k < F - 1:
                    acc[g] += part
                else:
                    kept = jnp.maximum(acc[g] + part, 0.0)
                    hidden[g] = (kept * kept).astype(BF16)

        def p_copy(s, u, g):
            i = (s * U + u) * 2 + g
            return remote(pbuf.at[s, u, g], srecv.at[s, u, g], ps + i, pr + i, tp=sib)

        def x_copy(s, u, g):
            td, i = s // Q, s % Q
            away = (x + X - td // 2) % X
            slot = (away + X - 1) % X % max(X - 1, 1)
            return remote(
                pbuf.at[s, u, g],
                xrecv.at[slot, g, i, u],
                xs + (s * U + u) * 2 + g,
                xr + ((slot * 2 + g) * Q + i) * U + u,
                tp=(td // 2) * 2 + c,
            )

        def z_copy(i, u):
            return remote(zsnd.at[i, u], zrecv.at[i, u], fz_s + i * U + u, fz_r + i * U + u, fs=partner)

        def unit(u):
            return (r + u) % U

        def low_order(k):
            if F != 4:
                return order(k)
            return (1 - deep) * order(k) + deep * order(DEEP_COLUMNS[k])

        def lower(k, u):
            s = low_order(k)
            if k == 0 and u == 0:
                for copy in loads[4 + n_small :]:
                    copy.wait()
            if k > 0 and u == U - 1:
                y_wait(down_stream, down_part, s)
            u = unit(u)
            td, i = s // Q, s % Q
            xd, cd = td // 2, td % 2
            for g in (1, 0):
                pf[g] = jnp.dot(hidden[g], dnb[s, u], preferred_element_type=F32)

                @pl.when(c != cd)
                def _():
                    pbuf[s, u, g] = pf[g].astype(BF16)
                    p_copy(s, u, g).start()

            @pl.when(c == cd)
            def _():
                for g in (1, 0):
                    p_copy(s, u, g).wait_recv()
                    total = pf[g] + srecv[s, u, g].astype(F32)

                    @pl.when(x == xd)
                    def _():
                        tot[g, i, u] = total

                    @pl.when(x != xd)
                    def _():
                        pbuf[s, u, g] = total.astype(BF16)
                        x_copy(s, u, g).start()

        def settle(k, u):
            s = low_order(k)
            u = unit(u)
            td, i = s // Q, s % Q

            @pl.when(td == t)
            def _():
                for g in (1, 0):
                    total = tot[g, i, u]
                    for slot in range(X - 1):
                        block = xrecv.at[slot, g, i, u]
                        remote(block, block, xs, xr + ((slot * 2 + g) * Q + i) * U + u, tp=sib).wait_recv()
                        total += xrecv[slot, g, i, u].astype(F32)
                    if g == 1:
                        zsnd[i, u] = total.astype(BF16)
                        z_copy(i, u).start()
                    else:
                        tot[0, i, u] = total

        def finish():
            for i in range(Q):
                for u in range(U):
                    z_copy(i, u).wait_recv()
                    base = i * dep + u * uc
                    columns = span(t * dc + base, uc, uc)
                    result[:, base : base + uc] = (
                        mid[0, :, columns].astype(F32) + (tot[0, i, u] + zrecv[i, u].astype(F32))
                    ).astype(BF16)

        streams = (
            (qkv_stream, qkv_part, qkv_own),
            (out_stream, out_part, out_own),
            (up_stream, up_part, up_own),
            (down_stream, down_part, down_own),
        )

        def passed(st, part, k):
            s = order(k)
            for ch in range(st.chunks):
                forward(st, part, s, ch, leave)
                for q in range(1, R):
                    y_copy(st, part, s, ch, q).wait_send()

        def summed(k):
            s = low_order(k)
            td = s // Q
            for u in range(U):
                for g in range(2):

                    @pl.when(c != td % 2)
                    def _():
                        p_copy(s, u, g).wait_send()

                    @pl.when((c == td % 2) & (x != td // 2))
                    def _():
                        x_copy(s, u, g).wait_send()

        def early_left():
            spread_drain(act_spread, act_block, act)
            for j in range(seqs):
                block = functools.partial(ret_block, j)
                spread_drain(ret_spread[j], block, block(t))
            spread_drain(mid_spread[0], mid_own, mid_own(t))
            spread_drain(mid_spread[1], mid_other, mid_other(t))
            to_partner.wait_send()
            for j in range(1, T):
                for i in range(Q):
                    om_copy(j, i).wait_send()
            for st, part, own in streams:
                along(st, part, own, leave)
                if not st.line:
                    across(st, part, own, leave)

            def sent(k, carry):
                for st, part, own in streams[:3]:
                    passed(st, part, k)
                return carry

            def sent_down(k, carry):
                passed(down_stream, down_part, k)
                return carry

            lax.fori_loop(1, F, sent, 0)
            lax.fori_loop(1, F - 1, sent_down, 0)
            for k in range(F - 2):
                summed(k)

        def late_left():
            passed(down_stream, down_part, F - 1)
            for k in range(F - 2, F):
                summed(k)
            for i in range(Q):
                for u in range(U):
                    z_copy(i, u).wait_send()

        near = deep == 0
        steps = {
            "begin": begin,
            "act": norm_act,
            "proj": project_with,
            "ret": retain,
            "mid": middle,
            "m0": lambda: norm_second(0),
            "tok": partner_rows,
            "m1": lambda: norm_second(1),
            "raise": raise_by,
            "low": lower,
            "set": settle,
            "left": early_left,
            "end": finish,
        }

        def small_on(k):
            pass_on(qkv_stream, qkv_part, k)
            pass_on(out_stream, out_part, k)

        moves = {
            "ps": small_on,
            "alu": lambda ch: along(up_stream, up_part, up_own, start, (ch,)),
            "acu": lambda ch: across(up_stream, up_part, up_own, start, (ch,)),
            "ald": lambda ch: along(down_stream, down_part, down_own, start, (ch,)),
            "acd": lambda ch: across(down_stream, down_part, down_own, start, (ch,)),
            "pu": lambda k, ch: pass_on(up_stream, up_part, k, (ch,)),
            "pd": lambda k, ch: pass_on(down_stream, down_part, k, (ch,)),
        }
        for name, *place in chain(F, U):
            steps[name](*place)
            for here, table in ((near, near_moves), (deep > 0, deep_moves)):
                todo = table.get((name, *place), ())
                if todo:

                    @pl.when(here)
                    def _():
                        for move, *which in todo:
                            moves[move](*which)

        late_left()

    vmem = pltpu.VMEM
    scratch = [
        vmem((n, D), BF16),
        vmem((n, D), BF16),
        vmem((D, 4 * hw), BF16),
        vmem((n, 4 * hw), F32),
        vmem((local_heads, SEQ_LEN, SEQ_LEN), F32),
        vmem((F, hw, dep), BF16),
        vmem((Q, T * hw, dep), BF16),
        vmem((T, n, hw), BF16),
        vmem((2, n, D), BF16),
        vmem((2, n, D), BF16),
        vmem((D, hid), BF16),
        vmem((F, U, hid, uc), BF16),
        vmem((2, n, hid), F32),
        vmem((2, n, hid), BF16),
        vmem((2, n, uc), F32),
        vmem((F, U, 2, n, uc), BF16),
        vmem((F, U, 2, n, uc), BF16),
        vmem((2, Q, U, n, uc), F32),
        vmem((max(X - 1, 1), 2, Q, U, n, uc), BF16),
        vmem((Q, U, n, uc), BF16),
        vmem((Q, U, n, uc), BF16),
        pltpu.SemaphoreType.DMA((plan.size,)),
    ]
    anywhere = pl.BlockSpec(memory_space=pl.ANY)
    in_vmem = pl.BlockSpec(memory_space=vmem)
    call = pl.pallas_call(
        kernel,
        name="layer",
        out_shape=jax.ShapeDtypeStruct((n, dc), BF16),
        in_specs=[anywhere] * (1 + n_small + 3) + [in_vmem] * 4 + [anywhere],
        out_specs=in_vmem,
        scratch_shapes=scratch,
        compiler_params=pltpu.CompilerParams(
            collective_id=0, has_side_effects=True, vmem_limit_bytes=62 * 1024 * 1024
        ),
    )
    return call, n_small


def solution(mesh):
    mesh_shape = dict(mesh.shape)

    def local(
        activations,
        norm_gain,
        query_weight,
        key_weight,
        value_weight,
        gate_weight,
        out_weight,
        mlp_gain,
        up_weight,
        down_weight,
    ):
        shapes = {
            "activations": activations.shape,
            "query_weight": query_weight.shape,
            "up_weight": up_weight.shape,
        }
        call, n_small = build(mesh_shape, shapes)
        small = (query_weight, key_weight, value_weight, gate_weight)
        if n_small == 1:
            small = (jnp.concatenate(small, axis=1),)
        cosine, sine, decay = tables(query_weight.shape[1])
        return call(
            activations,
            *small,
            out_weight,
            up_weight,
            down_weight,
            norm_gain.reshape(1, -1),
            mlp_gain.reshape(1, -1),
            jnp.asarray(cosine),
            jnp.asarray(sine),
            jnp.asarray(decay),
        )

    in_specs = (
        P(("rep", "fs"), "tp"),
        P(),
        P("fs", "tp"),
        P("fs", "tp"),
        P("fs", "tp"),
        P("fs", "tp"),
        P("tp", "fs"),
        P(),
        P("fs", "tp"),
        P("tp", "fs"),
    )
    return jax.shard_map(
        local, mesh=mesh, in_specs=in_specs, out_specs=P(("rep", "fs"), "tp"), check_vma=False
    )
```
